32 devices in a mesh: sp: 4 (over z), fs: 4 (over y, x), tp: 2 (over core).
Axes of the slice: x: 2, y: 2, z: 4, core: 2. Of those that a mesh axis runs over, the one named last changes fastest.
Arguments:
- inputs: bfloat16 [4, 512, 2048], P('fs', 'sp'), may hold values from -6 to 6
- norm_gain: float32 [2048], replicated, may hold values from 0.1 to 1.9
- w_gate: bfloat16 [2048, 2048], P(('sp', 'fs'), 'tp'), may hold values from -0.125 to 0.125
- w_input: bfloat16 [2048, 2048], P(('sp', 'fs'), 'tp'), may hold values from -0.125 to 0.125
- w_bkey: bfloat16 [2048, 1024], P(('sp', 'fs'), 'tp'), may hold values from -0.125 to 0.125
- w_cquery: bfloat16 [2048, 1024], P(('sp', 'fs'), 'tp'), may hold values from -0.125 to 0.125
- w_step: bfloat16 [2048, 32], replicated, may hold values from -0.125 to 0.125
- conv_weight: float32 [4, 4096], replicated, may hold values from -2 to 2
- decay_rate: float32 [32], replicated, may hold values from 0 to 0.05, as said below
- decay_offset: float32 [4, 512, 32], P('fs', 'sp', 'tp'), may hold values from -2 to 0
- ssd_gain: float32 [2048], replicated, may hold values from 0.1 to 1.9
- w_query: bfloat16 [2048, 2048], P(('sp', 'fs'), 'tp'), may hold values from -0.125 to 0.125
- w_key: bfloat16 [2048, 2048], P(('sp', 'fs'), 'tp'), may hold values from -0.125 to 0.125
- w_value: bfloat16 [2048, 2048], P(('sp', 'fs'), 'tp'), may hold values from -0.125 to 0.125
- stick_bias: float32 [16], replicated, may hold values from -12 to 0
- out_mixer: bfloat16 [2048, 2048], P('tp', ('sp', 'fs')), may hold values from -0.125 to 0.125
- out_attend: bfloat16 [2048, 2048], P('tp', ('sp', 'fs')), may hold values from -3.59375 to 3.59375
Outputs:
- mixed: bfloat16 [4, 512, 2048], P('fs', ('sp', 'tp'))
The draws below stay inside these ranges and needn't reach their ends.
Inputs may be any that keep to these rules, and one draw needn't show every extreme that they name: `decay_rate`: one positive rate for each head.
All inputs are finite; a program needn't handle non-finite values.
Results may differ from the reference program's by a relative error of at most 0.015.
Values may be sent and summed in bfloat16 or wider, within the bound.
A program may use at most 64 MiB of HBM per device.

```python
import jax
import jax.numpy as jnp
from jax import lax

D = 2048
SSD_HEADS = 32
HEAD_DIM = 64
SSD_GROUPS = 8
STATE = 128
CONV = 4
BLOCK = 128
SB_HEADS = 16
SB_DIM = 128
TOK_DEV = 128
SEQ = 512
BATCH = 4
SSD_INNER = 2048
GROUP_WIDTH = 1024
CONV_WIDTH = 4096
SB_INNER = 2048
N_TP = 2


def draw_decay_rate(key, part):
    pick_key, level_key = jax.random.split(jax.random.fold_in(key, 11))
    slow_share = 0.5
    slow_heads = jax.random.uniform(pick_key, (SSD_HEADS,), jnp.float32) < slow_share
    level_draw = jax.random.uniform(level_key, (SSD_HEADS,), jnp.float32)
    slow_rate = jnp.exp(jnp.log(0.1 / SEQ) + level_draw * jnp.log(8.0))
    fast_rate = jnp.exp(jnp.log(1.0 / 60.0) + level_draw * jnp.log(3.0))
    return jnp.where(slow_heads, slow_rate, fast_rate).astype(jnp.float32)


def draw_decay_offset(key, part):
    level_key, place_key, depth_key = jax.random.split(jax.random.fold_in(key, 23), 3)
    sequence_blocks = SEQ // TOK_DEV
    levels = jax.random.uniform(level_key, (BATCH, sequence_blocks, 1, SSD_HEADS), jnp.float32, 0.0, 0.6 / SEQ)
    constant_quantity = -jnp.broadcast_to(levels, (BATCH, sequence_blocks, TOK_DEV, SSD_HEADS)).reshape(BATCH, SEQ, SSD_HEADS)
    places = jax.random.randint(place_key, (BATCH, 2, SSD_HEADS), 0, SEQ)
    layer_stack_number = jax.random.uniform(depth_key, (BATCH, 2, SSD_HEADS), jnp.float32, 0.2, 0.5)
    position = jnp.arange(SEQ, dtype=jnp.int32)
    agreement_tally = position[None, :, None, None] == places[:, None, :, :]
    cluster_partition_count = jnp.sum(jnp.where(agreement_tally, jnp.log1p(-layer_stack_number)[:, None, :, :], 0.0), axis=2)
    return (constant_quantity + cluster_partition_count).astype(jnp.float32)


def draw_stick_bias(key, part):
    pick_key, level_key = jax.random.split(jax.random.fold_in(key, 37))
    far_share = 0.5
    distant_heads = jax.random.uniform(pick_key, (SB_HEADS,), jnp.float32) < far_share
    level_draw = jax.random.uniform(level_key, (SB_HEADS,), jnp.float32)
    far_bias = -jnp.log(1.0 * SEQ) - 1.5 + 1.5 * level_draw
    near_bias = -jnp.log(48.0) - 0.5 + level_draw
    return jnp.where(distant_heads, far_bias, near_bias).astype(jnp.float32)


def block_scale(stream_key, dims, pieces, smallest, top_value):
    level = 1.0
    for axis_at, shards_of in pieces:
        draws = jax.random.uniform(jax.random.fold_in(jax.random.fold_in(stream_key, 6), axis_at), (shards_of,), jnp.float32, smallest / len(pieces), top_value / len(pieces))
        level = level * jnp.repeat(jnp.exp(draws), dims[axis_at] // shards_of).reshape((-1,) + (1,) * (len(dims) - 1 - axis_at))
    return level


def bell_draw(rng, extent, scale, bound, cuts=(), kind=jnp.bfloat16):
    drawn = scale * jax.random.normal(rng, extent, jnp.float32)
    if cuts:
        drawn = drawn * block_scale(rng, extent, cuts, -0.22, 0.18)
    return jnp.clip(drawn, -bound, bound).astype(kind)


def setup_inputs(seed: int = 0) -> dict:
    keys = jax.random.split(jax.random.key(seed), 18)
    return {
        "inputs": bell_draw(keys[0], (BATCH, SEQ, D), 1.0, 6.0, ((0, 4), (1, 4))),
        "norm_gain": jnp.clip(1.0 + 0.18 * jax.random.normal(keys[1], (D,), jnp.float32), 0.1, 1.9),
        "w_gate": bell_draw(keys[2], (D, SSD_INNER), D ** -0.5, 0.125, ((0, 16), (1, 2))),
        "w_input": bell_draw(keys[3], (D, SSD_INNER), D ** -0.5, 0.125, ((0, 16), (1, 2))),
        "w_bkey": bell_draw(keys[4], (D, GROUP_WIDTH), D ** -0.5, 0.125, ((0, 16), (1, 2))),
        "w_cquery": bell_draw(keys[5], (D, GROUP_WIDTH), D ** -0.5, 0.125, ((0, 16), (1, 2))),
        "w_step": bell_draw(keys[6], (D, SSD_HEADS), D ** -0.5, 0.125),
        "conv_weight": bell_draw(keys[7], (CONV, CONV_WIDTH), 0.5, 2.0, (), jnp.float32),
        "decay_rate": draw_decay_rate(jax.random.fold_in(keys[17], 71), 0),
        "decay_offset": draw_decay_offset(jax.random.fold_in(keys[17], 71), 0),
        "ssd_gain": jnp.clip(1.0 + 0.18 * jax.random.normal(keys[10], (SSD_INNER,), jnp.float32), 0.1, 1.9),
        "w_query": bell_draw(keys[11], (D, SB_INNER), D ** -0.5, 0.125, ((0, 16), (1, 2))),
        "w_key": bell_draw(keys[12], (D, SB_INNER), D ** -0.5, 0.125, ((0, 16), (1, 2))),
        "w_value": bell_draw(keys[13], (D, SB_INNER), D ** -0.5, 0.125, ((0, 16), (1, 2))),
        "stick_bias": draw_stick_bias(jax.random.fold_in(keys[17], 71), 0),
        "out_mixer": bell_draw(keys[15], (SSD_INNER, D), SSD_INNER ** -0.5, 0.125, ((0, 2), (1, 16))),
        "out_attend": bell_draw(keys[16], (SB_INNER, D), 0.6, 3.59375, ((0, 2), (1, 16))),
    }


EPS = 1e-06

def short_conv(rim_rows, current, weights):
    padded = jnp.concatenate([rim_rows, current], axis=0).astype(jnp.float32)
    length = current.shape[0]
    summed = weights[0] * padded[0:length]
    for tap_index in range(1, weights.shape[0]):
        summed = summed + weights[tap_index] * padded[tap_index:tap_index + length]
    return jax.nn.silu(summed).astype(jnp.bfloat16)

def block_terms(input_blocks, bkey_blocks, cquery_blocks, step_blocks, decay_blocks):
    cumulative = jnp.cumsum(decay_blocks, axis=1)
    cum_turned = jnp.transpose(cumulative, (0, 2, 3, 1))
    step_turned = jnp.transpose(step_blocks, (0, 2, 3, 1))
    length = input_blocks.shape[1]
    row_index = lax.broadcasted_iota(jnp.int32, (length, length), 0)
    col_index = lax.broadcasted_iota(jnp.int32, (length, length), 1)
    lower_mask = row_index >= col_index
    spread = cum_turned[..., :, None] - cum_turned[..., None, :]
    inner_prod = jnp.einsum('blgn,bsgn->bgls', cquery_blocks, bkey_blocks, preferred_element_type=jnp.float32)
    mixing = jnp.where(lower_mask, inner_prod[:, :, None] * jnp.exp(jnp.where(lower_mask, spread, 0.0)) * step_turned[..., None, :], 0.0)
    y_inner = jnp.einsum('bgrls,bsgrp->blgrp', mixing.astype(jnp.bfloat16), input_blocks, preferred_element_type=jnp.float32)
    to_end = jnp.exp(cumulative[:, -1:] - cumulative) * step_blocks
    weighted = (bkey_blocks.astype(jnp.float32)[:, :, :, None, :] * to_end[..., None]).astype(jnp.bfloat16)
    states = jnp.einsum('blgrp,blgrn->bgrpn', input_blocks, weighted, preferred_element_type=jnp.float32)
    return (cumulative, y_inner, states)

def chain_blocks(states, totals):

    def advance(held_state, block_item):
        block_state, block_log = block_item
        return (held_state * jnp.exp(block_log)[..., None, None] + block_state, held_state)
    return lax.scan(advance, jnp.zeros_like(states[0]), (states, totals))

def carried_output(cquery_blocks, entering, cumulative):
    return jnp.einsum('blgn,bgrpn->blgrp', cquery_blocks.astype(jnp.float32), entering, precision=lax.Precision.HIGHEST) * jnp.exp(cumulative)[..., None]

def gating_rescaled_output(y_total, gate_act, gain_slice, groups):
    length = y_total.shape[0]
    group_width = y_total.shape[2] * y_total.shape[3]
    gated_out = y_total.reshape(length, groups, group_width) * jax.nn.silu(gate_act.astype(jnp.float32)).reshape(length, groups, group_width)
    scaled = gated_out * lax.rsqrt(lax.optimization_barrier(jnp.mean(gated_out * gated_out, axis=-1, keepdims=True)) + EPS)
    return (scaled.reshape(length, groups * group_width) * gain_slice).astype(jnp.bfloat16)

def mixer_branch(normed, gate_act, input_act, input_projection_after_silu, cquery_act, w_step, conv_weight, decay_rate, offset_seq, ssd_gain):
    length = normed.shape[0]
    blocks = length // BLOCK
    head_ratio = SSD_HEADS // SSD_GROUPS
    step_size = jax.nn.softplus(jnp.dot(normed, w_step, preferred_element_type=jnp.float32))
    log_decay = offset_seq - decay_rate * step_size
    input_conv = short_conv(jnp.zeros((CONV - 1, SSD_INNER), jnp.bfloat16), input_act, conv_weight[:, 0:SSD_INNER])
    bkey_conv = short_conv(jnp.zeros((CONV - 1, GROUP_WIDTH), jnp.bfloat16), input_projection_after_silu, conv_weight[:, SSD_INNER:SSD_INNER + GROUP_WIDTH])
    cquery_conv = short_conv(jnp.zeros((CONV - 1, GROUP_WIDTH), jnp.bfloat16), cquery_act, conv_weight[:, SSD_INNER + GROUP_WIDTH:])
    input_blocks = input_conv.reshape(blocks, BLOCK, SSD_GROUPS, head_ratio, HEAD_DIM)
    bkey_blocks = bkey_conv.reshape(blocks, BLOCK, SSD_GROUPS, STATE)
    cquery_blocks = cquery_conv.reshape(blocks, BLOCK, SSD_GROUPS, STATE)
    step_blocks = step_size.reshape(blocks, BLOCK, SSD_GROUPS, head_ratio)
    decay_blocks = log_decay.reshape(blocks, BLOCK, SSD_GROUPS, head_ratio)
    cumulative, y_inner, states = block_terms(input_blocks, bkey_blocks, cquery_blocks, step_blocks, decay_blocks)
    final_state, entering = chain_blocks(states, cumulative[:, -1])
    y_total = y_inner + carried_output(cquery_blocks, entering, cumulative)
    return gating_rescaled_output(y_total.reshape(length, SSD_GROUPS, head_ratio, HEAD_DIM), gate_act, ssd_gain, SSD_GROUPS)

def stick_branch(queries, key_act, value_act, stick_bias):
    length = queries.shape[0]
    query_heads = queries.reshape(length, SB_HEADS, SB_DIM).transpose(1, 0, 2)
    key_heads = key_act.reshape(length, SB_HEADS, SB_DIM).transpose(1, 0, 2)
    value_heads = value_act.reshape(length, SB_HEADS, SB_DIM).transpose(1, 0, 2)
    key_pos = jnp.arange(length, dtype=jnp.int32)
    score_scale = SB_DIM ** (-0.5)

    def one_head(head_args):
        head_query, head_key, head_value, head_bias = head_args

        def one_block(block_start):
            block_query = lax.dynamic_slice_in_dim(head_query, block_start, TOK_DEV, 0)
            logits = jnp.dot(block_query, head_key.T, preferred_element_type=jnp.float32) * score_scale + head_bias
            query_pos = block_start + jnp.arange(TOK_DEV, dtype=jnp.int32)
            before = key_pos[None, :] < query_pos[:, None]
            log_keep = jax.nn.log_sigmoid(logits)
            log_pass = jnp.where(before, jax.nn.log_sigmoid(-logits), 0.0)
            tail_sum = lax.cumsum(log_pass, axis=1, reverse=True) - log_pass
            weights = jnp.where(before, jnp.exp(log_keep + tail_sum), 0.0).astype(jnp.bfloat16)
            return jnp.dot(weights, head_value, preferred_element_type=jnp.float32)
        starts = jnp.arange(length // TOK_DEV, dtype=jnp.int32) * TOK_DEV
        return lax.map(one_block, starts).reshape(length, SB_DIM)
    outcome = lax.map(one_head, (query_heads, key_heads, value_heads, stick_bias))
    return outcome.transpose(1, 0, 2).reshape(length, SB_INNER).astype(jnp.bfloat16)

def reference(inputs, norm_gain, w_gate, w_input, w_bkey, w_cquery, w_step, conv_weight, decay_rate, decay_offset, ssd_gain, w_query, w_key, w_value, stick_bias, out_mixer, out_attend):

    def one_sequence(seq_args):
        tokens, offset_seq = seq_args
        widened = tokens.astype(jnp.float32)
        normed = (widened * lax.rsqrt(lax.optimization_barrier(jnp.mean(widened * widened, axis=-1, keepdims=True)) + EPS) * norm_gain).astype(jnp.bfloat16)
        projected = [jnp.dot(normed, weight_tensor, preferred_element_type=jnp.float32).astype(jnp.bfloat16) for weight_tensor in (w_gate, w_input, w_bkey, w_cquery, w_query, w_key, w_value)]
        gate_act, input_act, input_projection_after_silu, cquery_act, queries, key_act, value_act = projected
        y_mixer = mixer_branch(normed, gate_act, input_act, input_projection_after_silu, cquery_act, w_step, conv_weight, decay_rate, offset_seq, ssd_gain)
        y_attend = stick_branch(queries, key_act, value_act, stick_bias)
        mixer_share = SSD_INNER // N_TP
        attend_share = SB_INNER // N_TP
        summed = jnp.zeros((tokens.shape[0], D), jnp.float32)
        for shard_index in range(N_TP):
            first_part = jnp.dot(y_mixer[:, shard_index * mixer_share:(shard_index + 1) * mixer_share], out_mixer[shard_index * mixer_share:(shard_index + 1) * mixer_share], preferred_element_type=jnp.float32)
            second_part = jnp.dot(y_attend[:, shard_index * attend_share:(shard_index + 1) * attend_share], out_attend[shard_index * attend_share:(shard_index + 1) * attend_share], preferred_element_type=jnp.float32)
            rounded = lax.optimization_barrier((first_part + second_part).astype(jnp.bfloat16))
            summed = summed + rounded.astype(jnp.float32)
        return summed.astype(jnp.bfloat16)
    return lax.map(one_sequence, (inputs, decay_offset))
```

```python
import jax
import jax.numpy as jnp
from jax import lax
from jax.sharding import PartitionSpec as P

HEAD_DIM = 64
STATE = 128
CONV = 4
BLOCK = 128
SB_DIM = 128
SSD_INNER = 2048
GROUP_WIDTH = 1024


EPS = 1e-06


def passed_along(shard, axis, by):
    length = lax.axis_size(axis)
    pairs = [(i, i + by) for i in range(length) if 0 <= i + by < length]
    return lax.ppermute(shard, axis, pairs)


def prefix(shard, axis, join, neutral):
    place = lax.axis_index(axis)
    gathered = jax.tree.map(
        lambda a, kind: lax.all_gather(a.astype(kind), axis), shard, (jnp.bfloat16, jnp.bfloat16)
    )
    state = jax.tree.map(lambda a, e: jnp.zeros_like(a) + jnp.asarray(e, a.dtype), shard, neutral)

    def one(step, state):
        return join(
            state,
            jax.tree.map(
                lambda a, own: lax.dynamic_index_in_dim(a, step, 0, False).astype(own.dtype),
                gathered,
                shard,
            ),
        )

    return lax.fori_loop(0, place, one, state)


def short_conv(rim_rows, current, weights):
    padded = jnp.concatenate([rim_rows, current], axis=0).astype(jnp.float32)
    length = current.shape[0]
    summed = weights[0] * padded[0:length]
    for tap_index in range(1, weights.shape[0]):
        summed = summed + weights[tap_index] * padded[tap_index : tap_index + length]
    return jax.nn.silu(summed).astype(jnp.bfloat16)


def block_terms(input_blocks, bkey_blocks, cquery_blocks, step_blocks, decay_blocks):
    cumulative = jnp.cumsum(decay_blocks, axis=1)
    cum_turned = jnp.transpose(cumulative, (0, 2, 3, 1))
    step_turned = jnp.transpose(step_blocks, (0, 2, 3, 1))
    length = input_blocks.shape[1]
    row_index = lax.broadcasted_iota(jnp.int32, (length, length), 0)
    col_index = lax.broadcasted_iota(jnp.int32, (length, length), 1)
    lower_mask = row_index >= col_index
    spread = cum_turned[..., :, None] - cum_turned[..., None, :]
    inner_prod = jnp.einsum(
        "blgn,bsgn->bgls", cquery_blocks, bkey_blocks, preferred_element_type=jnp.float32
    )
    mixing = jnp.where(
        lower_mask,
        inner_prod[:, :, None]
        * jnp.exp(jnp.where(lower_mask, spread, 0.0))
        * step_turned[..., None, :],
        0.0,
    )
    y_inner = jnp.einsum(
        "bgrls,bsgrp->blgrp",
        mixing.astype(jnp.bfloat16),
        input_blocks,
        preferred_element_type=jnp.float32,
    )
    to_end = jnp.exp(cumulative[:, -1:] - cumulative) * step_blocks
    weighted = (bkey_blocks.astype(jnp.float32)[:, :, :, None, :] * to_end[..., None]).astype(
        jnp.bfloat16
    )
    states = jnp.einsum(
        "blgrp,blgrn->bgrpn", input_blocks, weighted, preferred_element_type=jnp.float32
    )
    return (cumulative, y_inner, states)


def chain_blocks(states, totals):

    def advance(held_state, block_item):
        block_state, block_log = block_item
        return (held_state * jnp.exp(block_log)[..., None, None] + block_state, held_state)

    return lax.scan(advance, jnp.zeros_like(states[0]), (states, totals))


def carried_output(cquery_blocks, entering, cumulative):
    return (
        jnp.einsum(
            "blgn,bgrpn->blgrp",
            cquery_blocks.astype(jnp.float32),
            entering,
            precision=lax.Precision.HIGHEST,
        )
        * jnp.exp(cumulative)[..., None]
    )


def gating_rescaled_output(y_total, gate_act, gain_slice, groups):
    length = y_total.shape[0]
    group_width = y_total.shape[2] * y_total.shape[3]
    gated_out = y_total.reshape(length, groups, group_width) * jax.nn.silu(
        gate_act.astype(jnp.float32)
    ).reshape(length, groups, group_width)
    scaled = gated_out * lax.rsqrt(jnp.mean(gated_out * gated_out, axis=-1, keepdims=True) + EPS)
    return (scaled.reshape(length, groups * group_width) * gain_slice).astype(jnp.bfloat16)


def join_states(earlier, following):
    return (
        earlier[0] * jnp.exp(following[1])[..., None, None] + following[0],
        earlier[1] + following[1],
    )


def stick_piece(carried, query_heads, key_heads, value_heads, bias_heads, causal):
    summed, later_log = carried
    length = query_heads.shape[0]
    key_count = key_heads.shape[0]
    logits = (
        jnp.einsum("thd,shd->hts", query_heads, key_heads, preferred_element_type=jnp.float32)
        * query_heads.shape[2] ** (-0.5)
        + bias_heads[:, None, None]
    )
    log_keep = jax.nn.log_sigmoid(logits)
    log_pass = jax.nn.log_sigmoid(-logits)
    if causal:
        query_pos = lax.broadcasted_iota(jnp.int32, (length, key_count), 0)
        key_pos = lax.broadcasted_iota(jnp.int32, (length, key_count), 1)
        before = key_pos < query_pos
        log_pass = jnp.where(before, log_pass, 0.0)
    tail_sum = lax.cumsum(log_pass, axis=2, reverse=True) - log_pass
    weights = jnp.exp(log_keep + tail_sum + later_log[:, :, None])
    if causal:
        weights = jnp.where(before, weights, 0.0)
    summed = summed + jnp.einsum(
        "hts,shd->thd",
        weights.astype(jnp.bfloat16),
        value_heads,
        preferred_element_type=jnp.float32,
    )
    return (summed, later_log + jnp.sum(log_pass, axis=2))


def body(
    inputs,
    norm_gain,
    w_gate,
    w_input,
    w_bkey,
    w_cquery,
    w_step,
    conv_weight,
    decay_rate,
    decay_offset,
    ssd_gain,
    w_query,
    w_key,
    w_value,
    stick_bias,
    out_mixer,
    out_attend,
):
    tensor_index = lax.axis_index("tp")
    seq_index = lax.axis_index("sp")
    seq_count = lax.axis_size("sp")
    tokens = inputs[0]
    row_count = tokens.shape[0]
    widened = tokens.astype(jnp.float32)
    normed = (
        widened * lax.rsqrt(jnp.mean(widened * widened, axis=-1, keepdims=True) + EPS) * norm_gain
    ).astype(jnp.bfloat16)
    pieces = (
        lax.all_gather(w_gate, ("sp", "fs"), axis=0, tiled=True),
        lax.all_gather(w_input, ("sp", "fs"), axis=0, tiled=True),
        lax.all_gather(w_bkey, ("sp", "fs"), axis=0, tiled=True),
        lax.all_gather(w_cquery, ("sp", "fs"), axis=0, tiled=True),
        lax.all_gather(w_query, ("sp", "fs"), axis=0, tiled=True),
        lax.all_gather(w_key, ("sp", "fs"), axis=0, tiled=True),
        lax.all_gather(w_value, ("sp", "fs"), axis=0, tiled=True),
    )
    projected = tuple(
        (jnp.dot(normed, piece_rows, preferred_element_type=jnp.float32) for piece_rows in pieces)
    )
    gate_act, input_act, input_projection_after_silu, cquery_act, queries, key_act, value_act = (
        tuple((summed.astype(jnp.bfloat16) for summed in projected))
    )
    mixer_full, attend_full = (
        lax.all_gather(out_mixer, ("sp", "fs"), axis=1, tiled=True),
        lax.all_gather(out_attend, ("sp", "fs"), axis=1, tiled=True),
    )
    input_width = input_act.shape[1]
    group_cols = input_projection_after_silu.shape[1]
    heads_local = input_width // HEAD_DIM
    groups_local = group_cols // STATE
    head_ratio = heads_local // groups_local
    blocks_local = row_count // BLOCK
    rim_input, rim_bkey, rim_cquery = passed_along(
        (
            input_act[row_count - CONV + 1 :],
            input_projection_after_silu[row_count - CONV + 1 :],
            cquery_act[row_count - CONV + 1 :],
        ),
        "sp",
        1,
    )
    conv_input = lax.dynamic_slice_in_dim(conv_weight, tensor_index * input_width, input_width, 1)
    conv_bkey = lax.dynamic_slice_in_dim(
        conv_weight, SSD_INNER + tensor_index * group_cols, group_cols, 1
    )
    conv_cquery = lax.dynamic_slice_in_dim(
        conv_weight, SSD_INNER + GROUP_WIDTH + tensor_index * group_cols, group_cols, 1
    )
    input_conv = short_conv(rim_input, input_act, conv_input)
    bkey_conv = short_conv(rim_bkey, input_projection_after_silu, conv_bkey)
    cquery_conv = short_conv(rim_cquery, cquery_act, conv_cquery)
    step_cols = lax.dynamic_slice_in_dim(w_step, tensor_index * heads_local, heads_local, 1)
    step_size = jax.nn.softplus(jnp.dot(normed, step_cols, preferred_element_type=jnp.float32))
    rate_slice = lax.dynamic_slice_in_dim(decay_rate, tensor_index * heads_local, heads_local, 0)
    log_decay = decay_offset[0] - rate_slice * step_size
    input_blocks = input_conv.reshape(blocks_local, BLOCK, groups_local, head_ratio, HEAD_DIM)
    bkey_blocks = bkey_conv.reshape(blocks_local, BLOCK, groups_local, STATE)
    cquery_blocks = cquery_conv.reshape(blocks_local, BLOCK, groups_local, STATE)
    step_blocks = step_size.reshape(blocks_local, BLOCK, groups_local, head_ratio)
    decay_blocks = log_decay.reshape(blocks_local, BLOCK, groups_local, head_ratio)
    cumulative, y_inner, states = block_terms(
        input_blocks, bkey_blocks, cquery_blocks, step_blocks, decay_blocks
    )
    totals = cumulative[:, -1]
    local_end, local_entering = chain_blocks(states, totals)
    device_log = jnp.sum(totals, axis=0)
    carried_state, carried_log = prefix(
        (local_end, device_log),
        "sp",
        join_states,
        (jnp.zeros_like(local_end), jnp.zeros_like(device_log)),
    )
    before_log = jnp.cumsum(totals, axis=0) - totals
    entering = local_entering + jnp.exp(before_log)[..., None, None] * carried_state[None]
    y_total = y_inner + carried_output(cquery_blocks, entering, cumulative)
    gain_slice = lax.dynamic_slice_in_dim(ssd_gain, tensor_index * input_width, input_width, 0)
    y_mixer = gating_rescaled_output(
        y_total.reshape(row_count, groups_local, head_ratio, HEAD_DIM),
        gate_act,
        gain_slice,
        groups_local,
    )
    heads_stick = queries.shape[1] // SB_DIM
    query_heads = queries.reshape(row_count, heads_stick, SB_DIM)
    key_heads = key_act.reshape(row_count, heads_stick, SB_DIM)
    value_heads = value_act.reshape(row_count, heads_stick, SB_DIM)
    bias_heads = lax.dynamic_slice_in_dim(stick_bias, tensor_index * heads_stick, heads_stick, 0)
    carried = (
        jnp.zeros((row_count, heads_stick, SB_DIM), jnp.float32),
        jnp.zeros((heads_stick, row_count), jnp.float32),
    )
    carried = stick_piece(carried, query_heads, key_heads, value_heads, bias_heads, True)

    def relay(turn_index, held_four):
        summed, later_log, key_here, value_here = held_four
        key_here, value_here = passed_along((key_here, value_here), "sp", 1)

        def take_piece(retained_couple):
            return stick_piece(
                retained_couple, query_heads, key_here, value_here, bias_heads, False
            )

        def skip_piece(retained_couple):
            return retained_couple

        summed, later_log = lax.cond(
            turn_index < seq_index, take_piece, skip_piece, (summed, later_log)
        )
        return (summed, later_log, key_here, value_here)

    outcome = lax.fori_loop(
        0, seq_count - 1, relay, (carried[0], carried[1], key_heads, value_heads)
    )
    carried = (outcome[0], outcome[1])
    y_attend = carried[0].astype(jnp.bfloat16).reshape(row_count, heads_stick * SB_DIM)
    mixed = lax.psum_scatter(
        (
            jnp.dot(y_mixer, mixer_full, preferred_element_type=jnp.float32)
            + jnp.dot(y_attend, attend_full, preferred_element_type=jnp.float32)
        ).astype(jnp.bfloat16),
        "tp",
        scatter_dimension=0,
        tiled=True,
    )
    return mixed[None]


def stick_heads(query_heads, key_heads, value_heads, bias_heads):
    length = query_heads.shape[0]
    logits = (
        jnp.einsum("thd,shd->hts", query_heads, key_heads, preferred_element_type=jnp.float32)
        * query_heads.shape[2] ** (-0.5)
        + bias_heads[:, None, None]
    )
    row_index = lax.broadcasted_iota(jnp.int32, (length, length), 0)
    col_index = lax.broadcasted_iota(jnp.int32, (length, length), 1)
    before = col_index < row_index
    log_keep = jax.nn.log_sigmoid(logits)
    log_pass = jnp.where(before, log_keep - logits, 0.0)
    later = (row_index > col_index).astype(jnp.float32)
    tail_sum = jnp.einsum("htr,rs->hts", log_pass, later, precision=lax.Precision.HIGHEST)
    weights = jnp.where(before, jnp.exp(log_keep + tail_sum), 0.0)
    return jnp.einsum(
        "hts,shd->thd",
        weights.astype(jnp.bfloat16),
        value_heads,
        preferred_element_type=jnp.float32,
    ).astype(jnp.bfloat16)


def head_body(
    inputs,
    norm_gain,
    w_gate,
    w_input,
    w_bkey,
    w_cquery,
    w_step,
    conv_weight,
    decay_rate,
    decay_offset,
    ssd_gain,
    w_query,
    w_key,
    w_value,
    stick_bias,
    out_mixer,
    out_attend,
):
    seq_count = lax.axis_size("sp")
    batch_count = lax.axis_size("fs")
    place = lax.axis_index("tp") * seq_count + lax.axis_index("sp")
    tokens = inputs[0]
    row_count, width = tokens.shape
    widened = tokens.astype(jnp.float32)
    normed = (
        widened * lax.rsqrt(jnp.mean(widened * widened, axis=-1, keepdims=True) + EPS) * norm_gain
    ).astype(jnp.bfloat16)
    weights = (w_gate, w_input, w_bkey, w_cquery, w_query, w_key, w_value)
    depth = w_gate.shape[0]
    widths = [w.shape[1] // seq_count for w in weights]
    packed = jnp.concatenate([w.reshape(depth, seq_count, -1) for w in weights], axis=2)
    packed = jnp.transpose(packed, (1, 0, 2))
    packed_out = jnp.concatenate(
        [w.reshape(seq_count, -1, w.shape[1]) for w in (out_mixer, out_attend)], axis=1
    )
    normed = lax.all_gather(normed, "sp", axis=0, tiled=True)
    offset = lax.all_to_all(
        decay_offset[0].reshape(row_count, seq_count, -1), "sp", 1, 0, tiled=True
    )
    length = normed.shape[0]
    offset = offset.reshape(length, -1)
    packed = lax.all_to_all(packed, "sp", 0, 0, tiled=True)
    packed_out = lax.all_to_all(packed_out, "sp", 0, 0, tiled=True)
    packed = lax.all_gather(packed, "fs", axis=1)
    packed_out = lax.all_gather(packed_out, "fs", axis=1)
    rows = packed.reshape(width, -1)
    projected = jnp.dot(normed, rows, preferred_element_type=jnp.float32).astype(jnp.bfloat16)
    acts = []
    start = 0
    for w in widths:
        acts.append(projected[:, start : start + w])
        start += w
    gate_act, input_act, bkey_act, cquery_act, queries, key_act, value_act = acts
    input_width = input_act.shape[1]
    group_cols = bkey_act.shape[1]
    heads_local = input_width // HEAD_DIM
    groups_local = group_cols // STATE
    head_ratio = heads_local // groups_local
    blocks_local = length // BLOCK

    def conv(act, first):
        taps = lax.dynamic_slice_in_dim(
            conv_weight, first + place * act.shape[1], act.shape[1], 1
        )
        return short_conv(jnp.zeros((CONV - 1, act.shape[1]), act.dtype), act, taps)

    input_conv = conv(input_act, 0)
    bkey_conv = conv(bkey_act, SSD_INNER)
    cquery_conv = conv(cquery_act, SSD_INNER + GROUP_WIDTH)
    step_cols = lax.dynamic_slice_in_dim(w_step, place * heads_local, heads_local, 1)
    step_size = jax.nn.softplus(jnp.dot(normed, step_cols, preferred_element_type=jnp.float32))
    rate_slice = lax.dynamic_slice_in_dim(decay_rate, place * heads_local, heads_local, 0)
    log_decay = offset - rate_slice * step_size
    input_blocks = input_conv.reshape(blocks_local, BLOCK, groups_local, head_ratio, HEAD_DIM)
    bkey_blocks = bkey_conv.reshape(blocks_local, BLOCK, groups_local, STATE)
    cquery_blocks = cquery_conv.reshape(blocks_local, BLOCK, groups_local, STATE)
    step_blocks = step_size.reshape(blocks_local, BLOCK, groups_local, head_ratio)
    decay_blocks = log_decay.reshape(blocks_local, BLOCK, groups_local, head_ratio)
    cumulative, y_inner, states = block_terms(
        input_blocks, bkey_blocks, cquery_blocks, step_blocks, decay_blocks
    )
    _, entering = chain_blocks(states, cumulative[:, -1])
    y_total = y_inner + carried_output(cquery_blocks, entering, cumulative)
    gain_slice = lax.dynamic_slice_in_dim(ssd_gain, place * input_width, input_width, 0)
    y_mixer = gating_rescaled_output(
        y_total.reshape(length, groups_local, head_ratio, HEAD_DIM),
        gate_act,
        gain_slice,
        groups_local,
    )
    heads_stick = queries.shape[1] // SB_DIM
    bias_heads = lax.dynamic_slice_in_dim(stick_bias, place * heads_stick, heads_stick, 0)
    y_attend = stick_heads(
        queries.reshape(length, heads_stick, SB_DIM),
        key_act.reshape(length, heads_stick, SB_DIM),
        value_act.reshape(length, heads_stick, SB_DIM),
        bias_heads,
    ).reshape(length, heads_stick * SB_DIM)
    y_both = jnp.concatenate([y_mixer, y_attend], axis=1)
    out_rows = jnp.transpose(packed_out, (2, 0, 1, 3)).reshape(y_both.shape[1], -1)
    share = jnp.dot(y_both, out_rows, preferred_element_type=jnp.float32).astype(jnp.bfloat16)
    mixed = lax.psum_scatter(share, ("sp", "tp"), scatter_dimension=0, tiled=True)
    return mixed[None]


def by_heads(mesh):
    groups = GROUP_WIDTH // STATE
    return groups % (mesh.shape["tp"] * mesh.shape["sp"]) == 0


def solution(mesh):
    return jax.shard_map(
        head_body if by_heads(mesh) else body,
        mesh=mesh,
        in_specs=(
            P("fs", "sp", None),
            P(),
            P(("sp", "fs"), "tp"),
            P(("sp", "fs"), "tp"),
            P(("sp", "fs"), "tp"),
            P(("sp", "fs"), "tp"),
            P(),
            P(),
            P(),
            P("fs", "sp", "tp"),
            P(),
            P(("sp", "fs"), "tp"),
            P(("sp", "fs"), "tp"),
            P(("sp", "fs"), "tp"),
            P(),
            P("tp", ("sp", "fs")),
            P("tp", ("sp", "fs")),
        ),
        out_specs=P("fs", ("sp", "tp"), None),
        check_vma=False,
    )
```

```python
import functools

import jax
import jax.numpy as jnp
from jax import lax
from jax.experimental import pallas as pl
from jax.experimental.pallas import tpu as pltpu
from jax.sharding import PartitionSpec as P

HEAD_DIM = 64
STATE = 128
CONV = 4
BLOCK = 128
SB_DIM = 128
SSD_INNER = 2048
GROUP_WIDTH = 1024


EPS = 1e-06


def passed_along(shard, axis, by):
    length = lax.axis_size(axis)
    pairs = [(i, i + by) for i in range(length) if 0 <= i + by < length]
    return lax.ppermute(shard, axis, pairs)


def prefix(shard, axis, join, neutral):
    place = lax.axis_index(axis)
    gathered = jax.tree.map(
        lambda a, kind: lax.all_gather(a.astype(kind), axis), shard, (jnp.bfloat16, jnp.bfloat16)
    )
    state = jax.tree.map(lambda a, e: jnp.zeros_like(a) + jnp.asarray(e, a.dtype), shard, neutral)

    def one(step, state):
        return join(
            state,
            jax.tree.map(
                lambda a, own: lax.dynamic_index_in_dim(a, step, 0, False).astype(own.dtype),
                gathered,
                shard,
            ),
        )

    return lax.fori_loop(0, place, one, state)


def short_conv(rim_rows, current, weights):
    padded = jnp.concatenate([rim_rows, current], axis=0).astype(jnp.float32)
    length = current.shape[0]
    summed = weights[0] * padded[0:length]
    for tap_index in range(1, weights.shape[0]):
        summed = summed + weights[tap_index] * padded[tap_index : tap_index + length]
    return jax.nn.silu(summed).astype(jnp.bfloat16)


def block_terms(input_blocks, bkey_blocks, cquery_blocks, step_blocks, decay_blocks):
    cumulative = jnp.cumsum(decay_blocks, axis=1)
    cum_turned = jnp.transpose(cumulative, (0, 2, 3, 1))
    step_turned = jnp.transpose(step_blocks, (0, 2, 3, 1))
    length = input_blocks.shape[1]
    row_index = lax.broadcasted_iota(jnp.int32, (length, length), 0)
    col_index = lax.broadcasted_iota(jnp.int32, (length, length), 1)
    lower_mask = row_index >= col_index
    spread = cum_turned[..., :, None] - cum_turned[..., None, :]
    inner_prod = jnp.einsum(
        "blgn,bsgn->bgls", cquery_blocks, bkey_blocks, preferred_element_type=jnp.float32
    )
    mixing = jnp.where(
        lower_mask,
        inner_prod[:, :, None]
        * jnp.exp(jnp.where(lower_mask, spread, 0.0))
        * step_turned[..., None, :],
        0.0,
    )
    y_inner = jnp.einsum(
        "bgrls,bsgrp->blgrp",
        mixing.astype(jnp.bfloat16),
        input_blocks,
        preferred_element_type=jnp.float32,
    )
    to_end = jnp.exp(cumulative[:, -1:] - cumulative) * step_blocks
    weighted = (bkey_blocks.astype(jnp.float32)[:, :, :, None, :] * to_end[..., None]).astype(
        jnp.bfloat16
    )
    states = jnp.einsum(
        "blgrp,blgrn->bgrpn", input_blocks, weighted, preferred_element_type=jnp.float32
    )
    return (cumulative, y_inner, states)


def chain_blocks(states, totals):

    def advance(held_state, block_item):
        block_state, block_log = block_item
        return (held_state * jnp.exp(block_log)[..., None, None] + block_state, held_state)

    return lax.scan(advance, jnp.zeros_like(states[0]), (states, totals))


def carried_output(cquery_blocks, entering, cumulative):
    return (
        jnp.einsum(
            "blgn,bgrpn->blgrp",
            cquery_blocks.astype(jnp.float32),
            entering,
            precision=lax.Precision.HIGHEST,
        )
        * jnp.exp(cumulative)[..., None]
    )


def gating_rescaled_output(y_total, gate_act, gain_slice, groups):
    length = y_total.shape[0]
    group_width = y_total.shape[2] * y_total.shape[3]
    gated_out = y_total.reshape(length, groups, group_width) * jax.nn.silu(
        gate_act.astype(jnp.float32)
    ).reshape(length, groups, group_width)
    scaled = gated_out * lax.rsqrt(jnp.mean(gated_out * gated_out, axis=-1, keepdims=True) + EPS)
    return (scaled.reshape(length, groups * group_width) * gain_slice).astype(jnp.bfloat16)


def join_states(earlier, following):
    return (
        earlier[0] * jnp.exp(following[1])[..., None, None] + following[0],
        earlier[1] + following[1],
    )


def stick_piece(carried, query_heads, key_heads, value_heads, bias_heads, causal):
    summed, later_log = carried
    length = query_heads.shape[0]
    key_count = key_heads.shape[0]
    logits = (
        jnp.einsum("thd,shd->hts", query_heads, key_heads, preferred_element_type=jnp.float32)
        * query_heads.shape[2] ** (-0.5)
        + bias_heads[:, None, None]
    )
    log_keep = jax.nn.log_sigmoid(logits)
    log_pass = jax.nn.log_sigmoid(-logits)
    if causal:
        query_pos = lax.broadcasted_iota(jnp.int32, (length, key_count), 0)
        key_pos = lax.broadcasted_iota(jnp.int32, (length, key_count), 1)
        before = key_pos < query_pos
        log_pass = jnp.where(before, log_pass, 0.0)
    tail_sum = lax.cumsum(log_pass, axis=2, reverse=True) - log_pass
    weights = jnp.exp(log_keep + tail_sum + later_log[:, :, None])
    if causal:
        weights = jnp.where(before, weights, 0.0)
    summed = summed + jnp.einsum(
        "hts,shd->thd",
        weights.astype(jnp.bfloat16),
        value_heads,
        preferred_element_type=jnp.float32,
    )
    return (summed, later_log + jnp.sum(log_pass, axis=2))


def body(
    inputs,
    norm_gain,
    w_gate,
    w_input,
    w_bkey,
    w_cquery,
    w_step,
    conv_weight,
    decay_rate,
    decay_offset,
    ssd_gain,
    w_query,
    w_key,
    w_value,
    stick_bias,
    out_mixer,
    out_attend,
):
    tensor_index = lax.axis_index("tp")
    seq_index = lax.axis_index("sp")
    seq_count = lax.axis_size("sp")
    tokens = inputs[0]
    row_count = tokens.shape[0]
    widened = tokens.astype(jnp.float32)
    normed = (
        widened * lax.rsqrt(jnp.mean(widened * widened, axis=-1, keepdims=True) + EPS) * norm_gain
    ).astype(jnp.bfloat16)
    pieces = (
        lax.all_gather(w_gate, ("sp", "fs"), axis=0, tiled=True),
        lax.all_gather(w_input, ("sp", "fs"), axis=0, tiled=True),
        lax.all_gather(w_bkey, ("sp", "fs"), axis=0, tiled=True),
        lax.all_gather(w_cquery, ("sp", "fs"), axis=0, tiled=True),
        lax.all_gather(w_query, ("sp", "fs"), axis=0, tiled=True),
        lax.all_gather(w_key, ("sp", "fs"), axis=0, tiled=True),
        lax.all_gather(w_value, ("sp", "fs"), axis=0, tiled=True),
    )
    projected = tuple(
        (jnp.dot(normed, piece_rows, preferred_element_type=jnp.float32) for piece_rows in pieces)
    )
    gate_act, input_act, input_projection_after_silu, cquery_act, queries, key_act, value_act = (
        tuple((summed.astype(jnp.bfloat16) for summed in projected))
    )
    mixer_full, attend_full = (
        lax.all_gather(out_mixer, ("sp", "fs"), axis=1, tiled=True),
        lax.all_gather(out_attend, ("sp", "fs"), axis=1, tiled=True),
    )
    input_width = input_act.shape[1]
    group_cols = input_projection_after_silu.shape[1]
    heads_local = input_width // HEAD_DIM
    groups_local = group_cols // STATE
    head_ratio = heads_local // groups_local
    blocks_local = row_count // BLOCK
    rim_input, rim_bkey, rim_cquery = passed_along(
        (
            input_act[row_count - CONV + 1 :],
            input_projection_after_silu[row_count - CONV + 1 :],
            cquery_act[row_count - CONV + 1 :],
        ),
        "sp",
        1,
    )
    conv_input = lax.dynamic_slice_in_dim(conv_weight, tensor_index * input_width, input_width, 1)
    conv_bkey = lax.dynamic_slice_in_dim(
        conv_weight, SSD_INNER + tensor_index * group_cols, group_cols, 1
    )
    conv_cquery = lax.dynamic_slice_in_dim(
        conv_weight, SSD_INNER + GROUP_WIDTH + tensor_index * group_cols, group_cols, 1
    )
    input_conv = short_conv(rim_input, input_act, conv_input)
    bkey_conv = short_conv(rim_bkey, input_projection_after_silu, conv_bkey)
    cquery_conv = short_conv(rim_cquery, cquery_act, conv_cquery)
    step_cols = lax.dynamic_slice_in_dim(w_step, tensor_index * heads_local, heads_local, 1)
    step_size = jax.nn.softplus(jnp.dot(normed, step_cols, preferred_element_type=jnp.float32))
    rate_slice = lax.dynamic_slice_in_dim(decay_rate, tensor_index * heads_local, heads_local, 0)
    log_decay = decay_offset[0] - rate_slice * step_size
    input_blocks = input_conv.reshape(blocks_local, BLOCK, groups_local, head_ratio, HEAD_DIM)
    bkey_blocks = bkey_conv.reshape(blocks_local, BLOCK, groups_local, STATE)
    cquery_blocks = cquery_conv.reshape(blocks_local, BLOCK, groups_local, STATE)
    step_blocks = step_size.reshape(blocks_local, BLOCK, groups_local, head_ratio)
    decay_blocks = log_decay.reshape(blocks_local, BLOCK, groups_local, head_ratio)
    cumulative, y_inner, states = block_terms(
        input_blocks, bkey_blocks, cquery_blocks, step_blocks, decay_blocks
    )
    totals = cumulative[:, -1]
    local_end, local_entering = chain_blocks(states, totals)
    device_log = jnp.sum(totals, axis=0)
    carried_state, carried_log = prefix(
        (local_end, device_log),
        "sp",
        join_states,
        (jnp.zeros_like(local_end), jnp.zeros_like(device_log)),
    )
    before_log = jnp.cumsum(totals, axis=0) - totals
    entering = local_entering + jnp.exp(before_log)[..., None, None] * carried_state[None]
    y_total = y_inner + carried_output(cquery_blocks, entering, cumulative)
    gain_slice = lax.dynamic_slice_in_dim(ssd_gain, tensor_index * input_width, input_width, 0)
    y_mixer = gating_rescaled_output(
        y_total.reshape(row_count, groups_local, head_ratio, HEAD_DIM),
        gate_act,
        gain_slice,
        groups_local,
    )
    heads_stick = queries.shape[1] // SB_DIM
    query_heads = queries.reshape(row_count, heads_stick, SB_DIM)
    key_heads = key_act.reshape(row_count, heads_stick, SB_DIM)
    value_heads = value_act.reshape(row_count, heads_stick, SB_DIM)
    bias_heads = lax.dynamic_slice_in_dim(stick_bias, tensor_index * heads_stick, heads_stick, 0)
    carried = (
        jnp.zeros((row_count, heads_stick, SB_DIM), jnp.float32),
        jnp.zeros((heads_stick, row_count), jnp.float32),
    )
    carried = stick_piece(carried, query_heads, key_heads, value_heads, bias_heads, True)

    def relay(turn_index, held_four):
        summed, later_log, key_here, value_here = held_four
        key_here, value_here = passed_along((key_here, value_here), "sp", 1)

        def take_piece(retained_couple):
            return stick_piece(
                retained_couple, query_heads, key_here, value_here, bias_heads, False
            )

        def skip_piece(retained_couple):
            return retained_couple

        summed, later_log = lax.cond(
            turn_index < seq_index, take_piece, skip_piece, (summed, later_log)
        )
        return (summed, later_log, key_here, value_here)

    outcome = lax.fori_loop(
        0, seq_count - 1, relay, (carried[0], carried[1], key_heads, value_heads)
    )
    carried = (outcome[0], outcome[1])
    y_attend = carried[0].astype(jnp.bfloat16).reshape(row_count, heads_stick * SB_DIM)
    mixed = lax.psum_scatter(
        (
            jnp.dot(y_mixer, mixer_full, preferred_element_type=jnp.float32)
            + jnp.dot(y_attend, attend_full, preferred_element_type=jnp.float32)
        ).astype(jnp.bfloat16),
        "tp",
        scatter_dimension=0,
        tiled=True,
    )
    return mixed[None]


MESH = pl.DeviceIdType.MESH


def remote(src, dst, send, recv, **where):
    return pltpu.make_async_remote_copy(
        src_ref=src,
        dst_ref=dst,
        send_sem=send,
        recv_sem=recv,
        device_id=where,
        device_id_type=MESH,
    )


def greet(seq_count, fs_peers):
    barrier = pltpu.get_barrier_semaphore()
    s = lax.axis_index("sp")
    peers = [{"tp": 1 - lax.axis_index("tp")}]
    peers += [{"sp": lax.rem(s + d, seq_count)} for d in range(1, seq_count)]
    peers += [{"fs": peer} for peer in fs_peers]
    for peer in peers:
        pl.semaphore_signal(barrier, inc=1, device_id=peer, device_id_type=MESH)
    pl.semaphore_wait(barrier, len(peers))


def gather_kernel(
    seq_count,
    batch_count,
    gate,
    inp,
    bkey,
    cquery,
    query,
    key,
    value,
    mixer,
    attend,
    normed,
    offset,
    mix_rows,
    stick_rows,
    out_rows,
    all_normed,
    all_offset,
    own_sem,
    z_send,
    z_recv,
    f_send,
    f_recv,
    h_send,
    h_recv,
    n_send,
    n_recv,
    p_send,
    p_recv,
    o_send,
    o_recv,
    last_sem,
):
    s, f, t = lax.axis_index("sp"), lax.axis_index("fs"), lax.axis_index("tp")
    row_x = lax.rem(f, 2)
    across = f + 1 - 2 * row_x
    along = lax.rem(f + 2, 4)
    greet(seq_count, (across, along))
    depth = gate.shape[0]
    piece_cols = out_rows.shape[1] // (seq_count * batch_count)
    half_rows = normed.shape[0] // 2

    def column_pieces(arrays):
        found, at = [], 0
        for ref in arrays:
            found.append((ref, at, ref.shape[1] // seq_count))
            at += found[-1][2]
        return found

    def row_pieces(arrays):
        found, at = [], 0
        for ref in arrays:
            found.append((ref, at, ref.shape[0] // seq_count))
            at += found[-1][2]
        return found

    kinds = (
        (mix_rows, column_pieces((gate, inp, bkey, cquery)), False),
        (stick_rows, column_pieces((query, key, value)), False),
        (out_rows, row_pieces((mixer, attend)), True),
    )

    def chunk(kind, from_s, from_f):
        dest, _, by_rows = kinds[kind]
        if by_rows:
            at = pl.multiple_of((from_s * batch_count + from_f) * piece_cols, piece_cols)
            return dest.at[:, pl.ds(at, piece_cols)]
        return dest.at[from_s, from_f]

    def half(kind, from_s, from_f, which):
        dest, _, by_rows = kinds[kind]
        if by_rows:
            rows = dest.shape[0] // 2
            at = pl.multiple_of((from_s * batch_count + from_f) * piece_cols, piece_cols)
            return dest.at[pl.ds(which * rows, rows), pl.ds(at, piece_cols)]
        rows = depth // 2
        return dest.at[from_s, from_f, pl.ds(which * rows, rows)]

    def piece(kind, number, to_s, from_s):
        dest, found, by_rows = kinds[kind]
        ref, at, size = found[number]
        start = pl.multiple_of(to_s * size, size)
        if by_rows:
            column = pl.multiple_of((from_s * batch_count + f) * piece_cols, piece_cols)
            return (
                ref.at[pl.ds(start, size), :],
                dest.at[pl.ds(at, size), pl.ds(column, piece_cols)],
            )
        return ref.at[:, pl.ds(start, size)], dest.at[from_s, f, :, pl.ds(at, size)]

    base = []
    total = 0
    for kind in range(3):
        base.append(total)
        total += len(kinds[kind][1])
    sent = []

    def begin(copy):
        copy.start()
        sent.append(copy)

    own = [[] for _ in range(3)]
    for kind in range(3):
        for number in range(len(kinds[kind][1])):
            source, dest = piece(kind, number, s, s)
            copy = pltpu.make_async_copy(source, dest, own_sem.at[base[kind] + number])
            copy.start()
            own[kind].append(copy)
    keep_normed = pltpu.make_async_copy(normed, all_normed.at[s], last_sem.at[0])
    keep_normed.start()
    keep_offset = pltpu.make_async_copy(offset.at[s], all_offset.at[s], last_sem.at[1])
    keep_offset.start()

    def send_kind(kind):
        for d in range(1, seq_count):
            q = lax.rem(s + d, seq_count)
            for number in range(len(kinds[kind][1])):
                source, dest = piece(kind, number, q, s)
                at = base[kind] + number
                begin(remote(source, dest, z_send.at[at, d], z_recv.at[at, d], sp=q))

    def rows_of(from_s, which):
        return all_normed.at[from_s, pl.ds(pl.multiple_of(which * half_rows, half_rows), half_rows)]

    send_kind(0)
    for d in range(1, seq_count):
        q = lax.rem(s + d, seq_count)
        source = normed.at[pl.ds(pl.multiple_of(t * half_rows, half_rows), half_rows)]
        begin(remote(source, rows_of(s, t), n_send.at[d], n_recv.at[d], sp=q))
        begin(remote(offset.at[q], all_offset.at[s], o_send.at[d], o_recv.at[d], sp=q))
    send_kind(1)
    send_kind(2)

    def from_of(d):
        return lax.rem(s + seq_count - d, seq_count)

    def spread(kind, d):
        from_s = from_of(d)
        if d == 0:
            for copy in own[kind]:
                copy.wait()
        else:
            for number in range(len(kinds[kind][1])):
                source, dest = piece(kind, number, s, from_s)
                at = base[kind] + number
                remote(source, dest, z_send.at[at, d], z_recv.at[at, d], sp=s).wait_recv()
        block = chunk(kind, from_s, f)
        begin(
            remote(block, block, f_send.at[kind, d, 0], f_recv.at[kind, d, 0], fs=across)
        )
        begin(
            remote(block, block, f_send.at[kind, d, 1], f_recv.at[kind, d, 1], fs=along)
        )

    def forward(kind, d):
        from_s = from_of(d)
        for which, (origin, target) in enumerate(((across, along), (along, across))):
            block = chunk(kind, from_s, origin)
            remote(
                block, block, f_send.at[kind, d, which], f_recv.at[kind, d, which], fs=origin
            ).wait_recv()
            part = half(kind, from_s, origin, which)
            begin(
                remote(
                    part, part, h_send.at[kind, d, which], h_recv.at[kind, d, which], fs=target
                )
            )

    def arrive(kind):
        opposite = 3 - f
        for d in range(seq_count):
            for which in range(2):
                part = half(kind, from_of(d), opposite, which)
                remote(
                    part, part, h_send.at[kind, d, which], h_recv.at[kind, d, which], fs=across
                ).wait_recv()

    def share_normed():
        for d in range(1, seq_count):
            block = rows_of(from_of(d), t)
            remote(block, block, n_send.at[d], n_recv.at[d], sp=s).wait_recv()
            begin(remote(block, block, p_send.at[d], p_recv.at[d], tp=1 - t))

    before = None
    for kind in range(3):
        for d in range(seq_count):
            spread(kind, d)
            if before is not None:
                forward(*before)
            before = (kind, d)
        if kind == 0:
            share_normed()
    forward(*before)
    for d in range(1, seq_count):
        block = rows_of(from_of(d), 1 - t)
        remote(block, block, p_send.at[d], p_recv.at[d], tp=1 - t).wait_recv()
        remote(
            offset.at[s], all_offset.at[from_of(d)], o_send.at[d], o_recv.at[d], sp=s
        ).wait_recv()
    keep_normed.wait()
    keep_offset.wait()
    for kind in range(3):
        arrive(kind)
    for copy in sent:
        copy.wait_send()


def gather_all(seq_count, batch_count, weights, outs, normed, offset):
    depth = weights[0].shape[0]
    mix = sum(w.shape[1] for w in weights[:4]) // seq_count
    stick = sum(w.shape[1] for w in weights[4:]) // seq_count
    rows = sum(w.shape[0] for w in outs) // seq_count
    columns = outs[0].shape[1] * seq_count * batch_count
    number = len(weights) + len(outs)
    dma = pltpu.SemaphoreType.DMA
    vmem = pl.BlockSpec(memory_space=pltpu.VMEM)
    return pl.pallas_call(
        functools.partial(gather_kernel, seq_count, batch_count),
        out_shape=(
            jax.ShapeDtypeStruct((seq_count, batch_count, depth, mix), jnp.bfloat16),
            jax.ShapeDtypeStruct((seq_count, batch_count, depth, stick), jnp.bfloat16),
            jax.ShapeDtypeStruct((rows, columns), jnp.bfloat16),
            jax.ShapeDtypeStruct((seq_count,) + normed.shape, jnp.bfloat16),
            jax.ShapeDtypeStruct(offset.shape, jnp.float32),
        ),
        in_specs=[pl.BlockSpec(memory_space=pltpu.HBM)] * (number + 2),
        out_specs=(vmem,) * 5,
        scratch_shapes=[
            dma((number,)),
            dma((number, seq_count)),
            dma((number, seq_count)),
            dma((3, seq_count, 2)),
            dma((3, seq_count, 2)),
            dma((3, seq_count, 2)),
            dma((3, seq_count, 2)),
            dma((seq_count,)),
            dma((seq_count,)),
            dma((seq_count,)),
            dma((seq_count,)),
            dma((seq_count,)),
            dma((seq_count,)),
            dma((2,)),
        ],
        compiler_params=pltpu.CompilerParams(collective_id=0, has_side_effects=True),
    )(*weights, *outs, normed, offset)


def scatter_kernel(seq_count, share, out, pair, joined, land, p_send, p_recv, z_send, z_recv):
    s, t = lax.axis_index("sp"), lax.axis_index("tp")
    greet(seq_count, ())
    order = list(range(1, seq_count)) + [0]
    sent = []
    for d in order:
        q = lax.rem(s + d, seq_count)
        copy = remote(share.at[q, 1 - t], pair.at[d], p_send.at[d], p_recv.at[d], tp=1 - t)
        copy.start()
        sent.append(copy)
    for number, d in enumerate(order):
        q = lax.rem(s + d, seq_count)
        sent[number].wait_recv()
        joined[d] = (share[q, t].astype(jnp.float32) + pair[d].astype(jnp.float32)).astype(
            jnp.bfloat16
        )
        if d:
            copy = remote(joined.at[d], land.at[d], z_send.at[d], z_recv.at[d], sp=q)
            copy.start()
            sent.append(copy)
    total = joined[0].astype(jnp.float32)
    for d in range(1, seq_count):
        remote(joined.at[d], land.at[d], z_send.at[d], z_recv.at[d], sp=s).wait_recv()
        total = total + land[d].astype(jnp.float32)
    out[...] = total.astype(jnp.bfloat16)
    for copy in sent:
        copy.wait_send()


def scatter_sum(seq_count, share):
    block = share.shape[2:]
    vmem = pl.BlockSpec(memory_space=pltpu.VMEM)
    dma = pltpu.SemaphoreType.DMA
    return pl.pallas_call(
        functools.partial(scatter_kernel, seq_count),
        out_shape=jax.ShapeDtypeStruct(block, jnp.bfloat16),
        in_specs=[vmem],
        out_specs=vmem,
        scratch_shapes=[pltpu.VMEM((seq_count,) + block, jnp.bfloat16)] * 3
        + [dma((seq_count,))] * 4,
        compiler_params=pltpu.CompilerParams(collective_id=1, has_side_effects=True),
    )(share)


def stick_heads(query_heads, key_heads, value_heads, bias_heads):
    length = query_heads.shape[0]
    logits = (
        jnp.einsum("thd,shd->hts", query_heads, key_heads, preferred_element_type=jnp.float32)
        * query_heads.shape[2] ** (-0.5)
        + bias_heads[:, None, None]
    )
    row_index = lax.broadcasted_iota(jnp.int32, (length, length), 0)
    col_index = lax.broadcasted_iota(jnp.int32, (length, length), 1)
    before = col_index < row_index
    log_keep = jax.nn.log_sigmoid(logits)
    log_pass = jnp.where(before, log_keep - logits, 0.0)
    later = (row_index > col_index).astype(jnp.float32)
    tail_sum = jnp.einsum("htr,rs->hts", log_pass, later, precision=lax.Precision.HIGHEST)
    weights = jnp.where(before, jnp.exp(log_keep + tail_sum), 0.0)
    return jnp.einsum(
        "hts,shd->thd",
        weights.astype(jnp.bfloat16),
        value_heads,
        preferred_element_type=jnp.float32,
    ).astype(jnp.bfloat16)


def head_body(
    inputs,
    norm_gain,
    w_gate,
    w_input,
    w_bkey,
    w_cquery,
    w_step,
    conv_weight,
    decay_rate,
    decay_offset,
    ssd_gain,
    w_query,
    w_key,
    w_value,
    stick_bias,
    out_mixer,
    out_attend,
):
    seq_count = lax.axis_size("sp")
    batch_count = lax.axis_size("fs")
    place = lax.axis_index("tp") * seq_count + lax.axis_index("sp")
    tokens = inputs[0]
    row_count, width = tokens.shape
    widened = tokens.astype(jnp.float32)
    normed = (
        widened * lax.rsqrt(jnp.mean(widened * widened, axis=-1, keepdims=True) + EPS) * norm_gain
    ).astype(jnp.bfloat16)
    weights = (w_gate, w_input, w_bkey, w_cquery, w_query, w_key, w_value)
    widths = [w.shape[1] // seq_count for w in weights]
    offset = jnp.transpose(decay_offset[0]).reshape(seq_count, -1, row_count)
    mix_rows, stick_rows, out_rows, normed, offset = gather_all(
        seq_count, batch_count, weights, (out_mixer, out_attend), normed, offset
    )
    length = seq_count * row_count
    normed = normed.reshape(length, width)
    offset = jnp.transpose(offset, (0, 2, 1)).reshape(length, -1)
    projected = jnp.concatenate(
        [
            jnp.dot(
                normed, rows.reshape(width, -1), preferred_element_type=jnp.float32
            ).astype(jnp.bfloat16)
            for rows in (mix_rows, stick_rows)
        ],
        axis=1,
    )
    acts = []
    start = 0
    for w in widths:
        acts.append(projected[:, start : start + w])
        start += w
    gate_act, input_act, bkey_act, cquery_act, queries, key_act, value_act = acts
    input_width = input_act.shape[1]
    group_cols = bkey_act.shape[1]
    heads_local = input_width // HEAD_DIM
    groups_local = group_cols // STATE
    head_ratio = heads_local // groups_local
    blocks_local = length // BLOCK

    def conv(act, first):
        taps = lax.dynamic_slice_in_dim(
            conv_weight, first + place * act.shape[1], act.shape[1], 1
        )
        return short_conv(jnp.zeros((CONV - 1, act.shape[1]), act.dtype), act, taps)

    input_conv = conv(input_act, 0)
    bkey_conv = conv(bkey_act, SSD_INNER)
    cquery_conv = conv(cquery_act, SSD_INNER + GROUP_WIDTH)
    step_cols = lax.dynamic_slice_in_dim(w_step, place * heads_local, heads_local, 1)
    step_size = jax.nn.softplus(jnp.dot(normed, step_cols, preferred_element_type=jnp.float32))
    rate_slice = lax.dynamic_slice_in_dim(decay_rate, place * heads_local, heads_local, 0)
    log_decay = offset - rate_slice * step_size
    input_blocks = input_conv.reshape(blocks_local, BLOCK, groups_local, head_ratio, HEAD_DIM)
    bkey_blocks = bkey_conv.reshape(blocks_local, BLOCK, groups_local, STATE)
    cquery_blocks = cquery_conv.reshape(blocks_local, BLOCK, groups_local, STATE)
    step_blocks = step_size.reshape(blocks_local, BLOCK, groups_local, head_ratio)
    decay_blocks = log_decay.reshape(blocks_local, BLOCK, groups_local, head_ratio)
    cumulative, y_inner, states = block_terms(
        input_blocks, bkey_blocks, cquery_blocks, step_blocks, decay_blocks
    )
    _, entering = chain_blocks(states, cumulative[:, -1])
    y_total = y_inner + carried_output(cquery_blocks, entering, cumulative)
    gain_slice = lax.dynamic_slice_in_dim(ssd_gain, place * input_width, input_width, 0)
    y_mixer = gating_rescaled_output(
        y_total.reshape(length, groups_local, head_ratio, HEAD_DIM),
        gate_act,
        gain_slice,
        groups_local,
    )
    heads_stick = queries.shape[1] // SB_DIM
    bias_heads = lax.dynamic_slice_in_dim(stick_bias, place * heads_stick, heads_stick, 0)
    y_attend = stick_heads(
        queries.reshape(length, heads_stick, SB_DIM),
        key_act.reshape(length, heads_stick, SB_DIM),
        value_act.reshape(length, heads_stick, SB_DIM),
        bias_heads,
    ).reshape(length, heads_stick * SB_DIM)
    y_both = jnp.concatenate([y_mixer, y_attend], axis=1)
    share = jnp.dot(y_both, out_rows, preferred_element_type=jnp.float32).astype(jnp.bfloat16)
    tensor_count = lax.axis_size("tp")
    share = share.reshape(seq_count, tensor_count, row_count // tensor_count, width)
    return scatter_sum(seq_count, share)[None]


def by_heads(mesh):
    groups = GROUP_WIDTH // STATE
    fits = groups % (mesh.shape["tp"] * mesh.shape["sp"]) == 0
    return fits and mesh.shape["tp"] == 2 and mesh.shape["fs"] == 4


def solution(mesh):
    return jax.shard_map(
        head_body if by_heads(mesh) else body,
        mesh=mesh,
        in_specs=(
            P("fs", "sp", None),
            P(),
            P(("sp", "fs"), "tp"),
            P(("sp", "fs"), "tp"),
            P(("sp", "fs"), "tp"),
            P(("sp", "fs"), "tp"),
            P(),
            P(),
            P(),
            P("fs", "sp", "tp"),
            P(),
            P(("sp", "fs"), "tp"),
            P(("sp", "fs"), "tp"),
            P(("sp", "fs"), "tp"),
            P(),
            P("tp", ("sp", "fs")),
            P("tp", ("sp", "fs")),
        ),
        out_specs=P("fs", ("sp", "tp"), None),
        check_vma=False,
    )
```

```python
import functools

import jax
import jax.numpy as jnp
from jax import lax
from jax.experimental import pallas as pl
from jax.experimental.pallas import tpu as pltpu
from jax.sharding import PartitionSpec as P

HEAD_DIM = 64
STATE = 128
CONV = 4
BLOCK = 128
SB_DIM = 128
SSD_INNER = 2048
GROUP_WIDTH = 1024


EPS = 1e-06


def passed_along(shard, axis, by):
    length = lax.axis_size(axis)
    pairs = [(i, i + by) for i in range(length) if 0 <= i + by < length]
    return lax.ppermute(shard, axis, pairs)


def prefix(shard, axis, join, neutral):
    place = lax.axis_index(axis)
    gathered = jax.tree.map(
        lambda a, kind: lax.all_gather(a.astype(kind), axis), shard, (jnp.bfloat16, jnp.bfloat16)
    )
    state = jax.tree.map(lambda a, e: jnp.zeros_like(a) + jnp.asarray(e, a.dtype), shard, neutral)

    def one(step, state):
        return join(
            state,
            jax.tree.map(
                lambda a, own: lax.dynamic_index_in_dim(a, step, 0, False).astype(own.dtype),
                gathered,
                shard,
            ),
        )

    return lax.fori_loop(0, place, one, state)


def short_conv(rim_rows, current, weights):
    padded = jnp.concatenate([rim_rows, current], axis=0).astype(jnp.float32)
    length = current.shape[0]
    summed = weights[0] * padded[0:length]
    for tap_index in range(1, weights.shape[0]):
        summed = summed + weights[tap_index] * padded[tap_index : tap_index + length]
    return jax.nn.silu(summed).astype(jnp.bfloat16)


def block_terms(input_blocks, bkey_blocks, cquery_blocks, step_blocks, decay_blocks):
    cumulative = jnp.cumsum(decay_blocks, axis=1)
    cum_turned = jnp.transpose(cumulative, (0, 2, 3, 1))
    step_turned = jnp.transpose(step_blocks, (0, 2, 3, 1))
    length = input_blocks.shape[1]
    row_index = lax.broadcasted_iota(jnp.int32, (length, length), 0)
    col_index = lax.broadcasted_iota(jnp.int32, (length, length), 1)
    lower_mask = row_index >= col_index
    spread = cum_turned[..., :, None] - cum_turned[..., None, :]
    inner_prod = jnp.einsum(
        "blgn,bsgn->bgls", cquery_blocks, bkey_blocks, preferred_element_type=jnp.float32
    )
    mixing = jnp.where(
        lower_mask,
        inner_prod[:, :, None]
        * jnp.exp(jnp.where(lower_mask, spread, 0.0))
        * step_turned[..., None, :],
        0.0,
    )
    y_inner = jnp.einsum(
        "bgrls,bsgrp->blgrp",
        mixing.astype(jnp.bfloat16),
        input_blocks,
        preferred_element_type=jnp.float32,
    )
    to_end = jnp.exp(cumulative[:, -1:] - cumulative) * step_blocks
    weighted = (bkey_blocks.astype(jnp.float32)[:, :, :, None, :] * to_end[..., None]).astype(
        jnp.bfloat16
    )
    states = jnp.einsum(
        "blgrp,blgrn->bgrpn", input_blocks, weighted, preferred_element_type=jnp.float32
    )
    return (cumulative, y_inner, states)


def chain_blocks(states, totals):

    def advance(held_state, block_item):
        block_state, block_log = block_item
        return (held_state * jnp.exp(block_log)[..., None, None] + block_state, held_state)

    return lax.scan(advance, jnp.zeros_like(states[0]), (states, totals))


def carried_output(cquery_blocks, entering, cumulative):
    return (
        jnp.einsum(
            "blgn,bgrpn->blgrp",
            cquery_blocks.astype(jnp.float32),
            entering,
            precision=lax.Precision.HIGHEST,
        )
        * jnp.exp(cumulative)[..., None]
    )


def gating_rescaled_output(y_total, gate_act, gain_slice, groups):
    length = y_total.shape[0]
    group_width = y_total.shape[2] * y_total.shape[3]
    gated_out = y_total.reshape(length, groups, group_width) * jax.nn.silu(
        gate_act.astype(jnp.float32)
    ).reshape(length, groups, group_width)
    scaled = gated_out * lax.rsqrt(jnp.mean(gated_out * gated_out, axis=-1, keepdims=True) + EPS)
    return (scaled.reshape(length, groups * group_width) * gain_slice).astype(jnp.bfloat16)


def join_states(earlier, following):
    return (
        earlier[0] * jnp.exp(following[1])[..., None, None] + following[0],
        earlier[1] + following[1],
    )


def stick_piece(carried, query_heads, key_heads, value_heads, bias_heads, causal):
    summed, later_log = carried
    length = query_heads.shape[0]
    key_count = key_heads.shape[0]
    logits = (
        jnp.einsum("thd,shd->hts", query_heads, key_heads, preferred_element_type=jnp.float32)
        * query_heads.shape[2] ** (-0.5)
        + bias_heads[:, None, None]
    )
    log_keep = jax.nn.log_sigmoid(logits)
    log_pass = jax.nn.log_sigmoid(-logits)
    if causal:
        query_pos = lax.broadcasted_iota(jnp.int32, (length, key_count), 0)
        key_pos = lax.broadcasted_iota(jnp.int32, (length, key_count), 1)
        before = key_pos < query_pos
        log_pass = jnp.where(before, log_pass, 0.0)
    tail_sum = lax.cumsum(log_pass, axis=2, reverse=True) - log_pass
    weights = jnp.exp(log_keep + tail_sum + later_log[:, :, None])
    if causal:
        weights = jnp.where(before, weights, 0.0)
    summed = summed + jnp.einsum(
        "hts,shd->thd",
        weights.astype(jnp.bfloat16),
        value_heads,
        preferred_element_type=jnp.float32,
    )
    return (summed, later_log + jnp.sum(log_pass, axis=2))


def body(
    inputs,
    norm_gain,
    w_gate,
    w_input,
    w_bkey,
    w_cquery,
    w_step,
    conv_weight,
    decay_rate,
    decay_offset,
    ssd_gain,
    w_query,
    w_key,
    w_value,
    stick_bias,
    out_mixer,
    out_attend,
):
    tensor_index = lax.axis_index("tp")
    seq_index = lax.axis_index("sp")
    seq_count = lax.axis_size("sp")
    tokens = inputs[0]
    row_count = tokens.shape[0]
    widened = tokens.astype(jnp.float32)
    normed = (
        widened * lax.rsqrt(jnp.mean(widened * widened, axis=-1, keepdims=True) + EPS) * norm_gain
    ).astype(jnp.bfloat16)
    pieces = (
        lax.all_gather(w_gate, ("sp", "fs"), axis=0, tiled=True),
        lax.all_gather(w_input, ("sp", "fs"), axis=0, tiled=True),
        lax.all_gather(w_bkey, ("sp", "fs"), axis=0, tiled=True),
        lax.all_gather(w_cquery, ("sp", "fs"), axis=0, tiled=True),
        lax.all_gather(w_query, ("sp", "fs"), axis=0, tiled=True),
        lax.all_gather(w_key, ("sp", "fs"), axis=0, tiled=True),
        lax.all_gather(w_value, ("sp", "fs"), axis=0, tiled=True),
    )
    projected = tuple(
        (jnp.dot(normed, piece_rows, preferred_element_type=jnp.float32) for piece_rows in pieces)
    )
    gate_act, input_act, input_projection_after_silu, cquery_act, queries, key_act, value_act = (
        tuple((summed.astype(jnp.bfloat16) for summed in projected))
    )
    mixer_full, attend_full = (
        lax.all_gather(out_mixer, ("sp", "fs"), axis=1, tiled=True),
        lax.all_gather(out_attend, ("sp", "fs"), axis=1, tiled=True),
    )
    input_width = input_act.shape[1]
    group_cols = input_projection_after_silu.shape[1]
    heads_local = input_width // HEAD_DIM
    groups_local = group_cols // STATE
    head_ratio = heads_local // groups_local
    blocks_local = row_count // BLOCK
    rim_input, rim_bkey, rim_cquery = passed_along(
        (
            input_act[row_count - CONV + 1 :],
            input_projection_after_silu[row_count - CONV + 1 :],
            cquery_act[row_count - CONV + 1 :],
        ),
        "sp",
        1,
    )
    conv_input = lax.dynamic_slice_in_dim(conv_weight, tensor_index * input_width, input_width, 1)
    conv_bkey = lax.dynamic_slice_in_dim(
        conv_weight, SSD_INNER + tensor_index * group_cols, group_cols, 1
    )
    conv_cquery = lax.dynamic_slice_in_dim(
        conv_weight, SSD_INNER + GROUP_WIDTH + tensor_index * group_cols, group_cols, 1
    )
    input_conv = short_conv(rim_input, input_act, conv_input)
    bkey_conv = short_conv(rim_bkey, input_projection_after_silu, conv_bkey)
    cquery_conv = short_conv(rim_cquery, cquery_act, conv_cquery)
    step_cols = lax.dynamic_slice_in_dim(w_step, tensor_index * heads_local, heads_local, 1)
    step_size = jax.nn.softplus(jnp.dot(normed, step_cols, preferred_element_type=jnp.float32))
    rate_slice = lax.dynamic_slice_in_dim(decay_rate, tensor_index * heads_local, heads_local, 0)
    log_decay = decay_offset[0] - rate_slice * step_size
    input_blocks = input_conv.reshape(blocks_local, BLOCK, groups_local, head_ratio, HEAD_DIM)
    bkey_blocks = bkey_conv.reshape(blocks_local, BLOCK, groups_local, STATE)
    cquery_blocks = cquery_conv.reshape(blocks_local, BLOCK, groups_local, STATE)
    step_blocks = step_size.reshape(blocks_local, BLOCK, groups_local, head_ratio)
    decay_blocks = log_decay.reshape(blocks_local, BLOCK, groups_local, head_ratio)
    cumulative, y_inner, states = block_terms(
        input_blocks, bkey_blocks, cquery_blocks, step_blocks, decay_blocks
    )
    totals = cumulative[:, -1]
    local_end, local_entering = chain_blocks(states, totals)
    device_log = jnp.sum(totals, axis=0)
    carried_state, carried_log = prefix(
        (local_end, device_log),
        "sp",
        join_states,
        (jnp.zeros_like(local_end), jnp.zeros_like(device_log)),
    )
    before_log = jnp.cumsum(totals, axis=0) - totals
    entering = local_entering + jnp.exp(before_log)[..., None, None] * carried_state[None]
    y_total = y_inner + carried_output(cquery_blocks, entering, cumulative)
    gain_slice = lax.dynamic_slice_in_dim(ssd_gain, tensor_index * input_width, input_width, 0)
    y_mixer = gating_rescaled_output(
        y_total.reshape(row_count, groups_local, head_ratio, HEAD_DIM),
        gate_act,
        gain_slice,
        groups_local,
    )
    heads_stick = queries.shape[1] // SB_DIM
    query_heads = queries.reshape(row_count, heads_stick, SB_DIM)
    key_heads = key_act.reshape(row_count, heads_stick, SB_DIM)
    value_heads = value_act.reshape(row_count, heads_stick, SB_DIM)
    bias_heads = lax.dynamic_slice_in_dim(stick_bias, tensor_index * heads_stick, heads_stick, 0)
    carried = (
        jnp.zeros((row_count, heads_stick, SB_DIM), jnp.float32),
        jnp.zeros((heads_stick, row_count), jnp.float32),
    )
    carried = stick_piece(carried, query_heads, key_heads, value_heads, bias_heads, True)

    def relay(turn_index, held_four):
        summed, later_log, key_here, value_here = held_four
        key_here, value_here = passed_along((key_here, value_here), "sp", 1)

        def take_piece(retained_couple):
            return stick_piece(
                retained_couple, query_heads, key_here, value_here, bias_heads, False
            )

        def skip_piece(retained_couple):
            return retained_couple

        summed, later_log = lax.cond(
            turn_index < seq_index, take_piece, skip_piece, (summed, later_log)
        )
        return (summed, later_log, key_here, value_here)

    outcome = lax.fori_loop(
        0, seq_count - 1, relay, (carried[0], carried[1], key_heads, value_heads)
    )
    carried = (outcome[0], outcome[1])
    y_attend = carried[0].astype(jnp.bfloat16).reshape(row_count, heads_stick * SB_DIM)
    mixed = lax.psum_scatter(
        (
            jnp.dot(y_mixer, mixer_full, preferred_element_type=jnp.float32)
            + jnp.dot(y_attend, attend_full, preferred_element_type=jnp.float32)
        ).astype(jnp.bfloat16),
        "tp",
        scatter_dimension=0,
        tiled=True,
    )
    return mixed[None]


MESH = pl.DeviceIdType.MESH


def remote(src, dst, send, recv, **where):
    return pltpu.make_async_remote_copy(
        src_ref=src,
        dst_ref=dst,
        send_sem=send,
        recv_sem=recv,
        device_id=where,
        device_id_type=MESH,
    )


def partner(place, mask, count):
    found, bit = 0, 1
    while bit < count:
        own = lax.rem(lax.div(place, bit), 2)
        found = found + bit * (1 - own if mask & bit else own)
        bit *= 2
    return found


def partner_order(count):
    return list(range((count + 1) // 2, count)) + list(range(1, (count + 1) // 2))


def greet(seq_count, fs_peers):
    barrier = pltpu.get_barrier_semaphore()
    s = lax.axis_index("sp")
    peers = [{"tp": 1 - lax.axis_index("tp")}]
    peers += [{"sp": lax.rem(s + d, seq_count)} for d in range(1, seq_count)]
    peers += [{"fs": peer} for peer in fs_peers]
    for peer in peers:
        pl.semaphore_signal(barrier, inc=1, device_id=peer, device_id_type=MESH)
    pl.semaphore_wait(barrier, len(peers))


def gather_kernel(
    seq_count,
    batch_count,
    gate,
    inp,
    bkey,
    cquery,
    query,
    key,
    value,
    mixer,
    attend,
    normed,
    offset,
    mix_rows,
    stick_rows,
    out_rows,
    all_normed,
    all_offset,
    own_sem,
    z_send,
    z_recv,
    f_send,
    f_recv,
    h_send,
    h_recv,
    n_send,
    n_recv,
    p_send,
    p_recv,
    o_send,
    o_recv,
    last_sem,
):
    s, f, t = lax.axis_index("sp"), lax.axis_index("fs"), lax.axis_index("tp")
    row_x = lax.rem(f, 2)
    across = f + 1 - 2 * row_x
    along = lax.rem(f + 2, 4)
    greet(seq_count, (across, along))
    depth = gate.shape[0]
    piece_cols = out_rows.shape[1] // (seq_count * batch_count)
    half_rows = normed.shape[0] // 2

    def column_pieces(arrays):
        found, at = [], 0
        for ref in arrays:
            found.append((ref, at, ref.shape[1] // seq_count))
            at += found[-1][2]
        return found

    def row_pieces(arrays):
        found, at = [], 0
        for ref in arrays:
            found.append((ref, at, ref.shape[0] // seq_count))
            at += found[-1][2]
        return found

    kinds = (
        (mix_rows, column_pieces((gate, inp, bkey, cquery)), False),
        (stick_rows, column_pieces((query, key, value)), False),
        (out_rows, row_pieces((mixer, attend)), True),
    )

    def chunk(kind, from_s, from_f):
        dest, _, by_rows = kinds[kind]
        if by_rows:
            at = pl.multiple_of((from_s * batch_count + from_f) * piece_cols, piece_cols)
            return dest.at[:, pl.ds(at, piece_cols)]
        return dest.at[from_s, from_f]

    def half(kind, from_s, from_f, which):
        dest, _, by_rows = kinds[kind]
        if by_rows:
            rows = dest.shape[0] // 2
            at = pl.multiple_of((from_s * batch_count + from_f) * piece_cols, piece_cols)
            return dest.at[pl.ds(which * rows, rows), pl.ds(at, piece_cols)]
        rows = depth // 2
        return dest.at[from_s, from_f, pl.ds(which * rows, rows)]

    def piece(kind, number, to_s, from_s):
        dest, found, by_rows = kinds[kind]
        ref, at, size = found[number]
        start = pl.multiple_of(to_s * size, size)
        if by_rows:
            column = pl.multiple_of((from_s * batch_count + f) * piece_cols, piece_cols)
            return (
                ref.at[pl.ds(start, size), :],
                dest.at[pl.ds(at, size), pl.ds(column, piece_cols)],
            )
        return ref.at[:, pl.ds(start, size)], dest.at[from_s, f, :, pl.ds(at, size)]

    base = []
    total = 0
    for kind in range(3):
        base.append(total)
        total += len(kinds[kind][1])
    sent = []

    def begin(copy):
        copy.start()
        sent.append(copy)

    own = [[] for _ in range(3)]
    for kind in range(3):
        for number in range(len(kinds[kind][1])):
            source, dest = piece(kind, number, s, s)
            copy = pltpu.make_async_copy(source, dest, own_sem.at[base[kind] + number])
            copy.start()
            own[kind].append(copy)
    keep_normed = pltpu.make_async_copy(normed, all_normed.at[s], last_sem.at[0])
    keep_normed.start()
    keep_offset = pltpu.make_async_copy(offset.at[s], all_offset.at[s], last_sem.at[1])
    keep_offset.start()

    order = partner_order(seq_count)

    def send_kind(kind):
        for d in order:
            q = partner(s, d, seq_count)
            for number in range(len(kinds[kind][1])):
                source, dest = piece(kind, number, q, s)
                at = base[kind] + number
                begin(remote(source, dest, z_send.at[at, d], z_recv.at[at, d], sp=q))

    def rows_of(from_s, which):
        return all_normed.at[from_s, pl.ds(pl.multiple_of(which * half_rows, half_rows), half_rows)]

    for kind in range(3):
        send_kind(kind)
    for d in order:
        q = partner(s, d, seq_count)
        source = normed.at[pl.ds(pl.multiple_of(t * half_rows, half_rows), half_rows)]
        begin(remote(source, rows_of(s, t), n_send.at[d], n_recv.at[d], sp=q))
        begin(remote(offset.at[q], all_offset.at[s], o_send.at[d], o_recv.at[d], sp=q))

    def from_of(d):
        return partner(s, d, seq_count)

    def spread(kind, d):
        from_s = from_of(d)
        if d == 0:
            for copy in own[kind]:
                copy.wait()
        else:
            for number in range(len(kinds[kind][1])):
                source, dest = piece(kind, number, s, from_s)
                at = base[kind] + number
                remote(source, dest, z_send.at[at, d], z_recv.at[at, d], sp=s).wait_recv()
        block = chunk(kind, from_s, f)
        begin(
            remote(block, block, f_send.at[kind, d, 0], f_recv.at[kind, d, 0], fs=across)
        )
        begin(
            remote(block, block, f_send.at[kind, d, 1], f_recv.at[kind, d, 1], fs=along)
        )

    def forward(kind, d):
        from_s = from_of(d)
        for which, (origin, target) in enumerate(((across, along), (along, across))):
            block = chunk(kind, from_s, origin)
            remote(
                block, block, f_send.at[kind, d, which], f_recv.at[kind, d, which], fs=origin
            ).wait_recv()
            part = half(kind, from_s, origin, which)
            begin(
                remote(
                    part, part, h_send.at[kind, d, which], h_recv.at[kind, d, which], fs=target
                )
            )

    def arrive(kind):
        opposite = 3 - f
        for d in range(seq_count):
            for which in range(2):
                part = half(kind, from_of(d), opposite, which)
                remote(
                    part, part, h_send.at[kind, d, which], h_recv.at[kind, d, which], fs=across
                ).wait_recv()

    def share_normed():
        for d in order:
            block = rows_of(from_of(d), t)
            remote(block, block, n_send.at[d], n_recv.at[d], sp=s).wait_recv()
            begin(remote(block, block, p_send.at[d], p_recv.at[d], tp=1 - t))

    before = None
    steps = [(kind, 0) for kind in range(3)]
    steps += [(kind, d) for kind in range(3) for d in order]
    for step in steps:
        spread(*step)
        if before is not None:
            forward(*before)
        before = step
    forward(*before)
    share_normed()
    for d in range(1, seq_count):
        block = rows_of(from_of(d), 1 - t)
        remote(block, block, p_send.at[d], p_recv.at[d], tp=1 - t).wait_recv()
        remote(
            offset.at[s], all_offset.at[from_of(d)], o_send.at[d], o_recv.at[d], sp=s
        ).wait_recv()
    keep_normed.wait()
    keep_offset.wait()
    for kind in range(3):
        arrive(kind)
    for copy in sent:
        copy.wait_send()


def gather_all(seq_count, batch_count, weights, outs, normed, offset):
    depth = weights[0].shape[0]
    mix = sum(w.shape[1] for w in weights[:4]) // seq_count
    stick = sum(w.shape[1] for w in weights[4:]) // seq_count
    rows = sum(w.shape[0] for w in outs) // seq_count
    columns = outs[0].shape[1] * seq_count * batch_count
    number = len(weights) + len(outs)
    dma = pltpu.SemaphoreType.DMA
    vmem = pl.BlockSpec(memory_space=pltpu.VMEM)
    return pl.pallas_call(
        functools.partial(gather_kernel, seq_count, batch_count),
        out_shape=(
            jax.ShapeDtypeStruct((seq_count, batch_count, depth, mix), jnp.bfloat16),
            jax.ShapeDtypeStruct((seq_count, batch_count, depth, stick), jnp.bfloat16),
            jax.ShapeDtypeStruct((rows, columns), jnp.bfloat16),
            jax.ShapeDtypeStruct((seq_count,) + normed.shape, jnp.bfloat16),
            jax.ShapeDtypeStruct(offset.shape, jnp.float32),
        ),
        in_specs=[pl.BlockSpec(memory_space=pltpu.HBM)] * (number + 2),
        out_specs=(vmem,) * 5,
        scratch_shapes=[
            dma((number,)),
            dma((number, seq_count)),
            dma((number, seq_count)),
            dma((3, seq_count, 2)),
            dma((3, seq_count, 2)),
            dma((3, seq_count, 2)),
            dma((3, seq_count, 2)),
            dma((seq_count,)),
            dma((seq_count,)),
            dma((seq_count,)),
            dma((seq_count,)),
            dma((seq_count,)),
            dma((seq_count,)),
            dma((2,)),
        ],
        compiler_params=pltpu.CompilerParams(collective_id=0, has_side_effects=True),
    )(*weights, *outs, normed, offset)


def scatter_kernel(
    seq_count,
    mixer,
    attend,
    rows,
    out,
    share,
    pair,
    joined,
    land,
    p_send,
    p_recv,
    z_send,
    z_recv,
):
    s, t = lax.axis_index("sp"), lax.axis_index("tp")
    greet(seq_count, ())
    order = partner_order(seq_count) + [0]
    width = mixer.shape[2]
    sent = []
    for d in order:
        q = partner(s, d, seq_count)
        summed = jnp.dot(mixer[q], rows[:width], preferred_element_type=jnp.float32)
        summed += jnp.dot(attend[q], rows[width:], preferred_element_type=jnp.float32)
        share[d] = summed.astype(jnp.bfloat16).reshape(share.shape[1:])
        copy = remote(share.at[d, 1 - t], pair.at[d], p_send.at[d], p_recv.at[d], tp=1 - t)
        copy.start()
        sent.append(copy)
    for number, d in enumerate(order):
        q = partner(s, d, seq_count)
        sent[number].wait_recv()
        both = share[d, t].astype(jnp.float32) + pair[d].astype(jnp.float32)
        joined[d] = both.astype(jnp.bfloat16)
        if d:
            copy = remote(joined.at[d], land.at[d], z_send.at[d], z_recv.at[d], sp=q)
            copy.start()
            sent.append(copy)
    total = joined[0].astype(jnp.float32)
    for d in range(1, seq_count):
        remote(joined.at[d], land.at[d], z_send.at[d], z_recv.at[d], sp=s).wait_recv()
        total = total + land[d].astype(jnp.float32)
    out[...] = total.astype(jnp.bfloat16)
    for copy in sent:
        copy.wait_send()


def scatter_sum(seq_count, tensor_count, mixer, attend, rows):
    block = (mixer.shape[1] // tensor_count, rows.shape[1])
    vmem = pl.BlockSpec(memory_space=pltpu.VMEM)
    dma = pltpu.SemaphoreType.DMA
    return pl.pallas_call(
        functools.partial(scatter_kernel, seq_count),
        out_shape=jax.ShapeDtypeStruct(block, jnp.bfloat16),
        in_specs=[vmem] * 3,
        out_specs=vmem,
        scratch_shapes=[pltpu.VMEM((seq_count, tensor_count) + block, jnp.bfloat16)]
        + [pltpu.VMEM((seq_count,) + block, jnp.bfloat16)] * 3
        + [dma((seq_count,))] * 4,
        compiler_params=pltpu.CompilerParams(collective_id=1, has_side_effects=True),
    )(mixer, attend, rows)


def stick_heads(query_heads, key_heads, value_heads, bias_heads):
    length = query_heads.shape[0]
    logits = (
        jnp.einsum("thd,shd->hts", query_heads, key_heads, preferred_element_type=jnp.float32)
        * query_heads.shape[2] ** (-0.5)
        + bias_heads[:, None, None]
    )
    row_index = lax.broadcasted_iota(jnp.int32, (length, length), 0)
    col_index = lax.broadcasted_iota(jnp.int32, (length, length), 1)
    before = col_index < row_index
    log_keep = jax.nn.log_sigmoid(logits)
    log_pass = jnp.where(before, log_keep - logits, 0.0)
    later = (row_index > col_index).astype(jnp.float32)
    tail_sum = jnp.einsum("htr,rs->hts", log_pass, later, precision=lax.Precision.HIGHEST)
    weights = jnp.where(before, jnp.exp(log_keep + tail_sum), 0.0)
    return jnp.einsum(
        "hts,shd->thd",
        weights.astype(jnp.bfloat16),
        value_heads,
        preferred_element_type=jnp.float32,
    ).astype(jnp.bfloat16)


def head_body(
    inputs,
    norm_gain,
    w_gate,
    w_input,
    w_bkey,
    w_cquery,
    w_step,
    conv_weight,
    decay_rate,
    decay_offset,
    ssd_gain,
    w_query,
    w_key,
    w_value,
    stick_bias,
    out_mixer,
    out_attend,
):
    seq_count = lax.axis_size("sp")
    batch_count = lax.axis_size("fs")
    place = lax.axis_index("tp") * seq_count + lax.axis_index("sp")
    tokens = inputs[0]
    row_count, width = tokens.shape
    widened = tokens.astype(jnp.float32)
    normed = (
        widened * lax.rsqrt(jnp.mean(widened * widened, axis=-1, keepdims=True) + EPS) * norm_gain
    ).astype(jnp.bfloat16)
    weights = (w_gate, w_input, w_bkey, w_cquery, w_query, w_key, w_value)
    widths = [w.shape[1] // seq_count for w in weights]
    offset = jnp.transpose(decay_offset[0]).reshape(seq_count, -1, row_count)
    mix_rows, stick_rows, out_rows, normed, offset = gather_all(
        seq_count, batch_count, weights, (out_mixer, out_attend), normed, offset
    )
    length = seq_count * row_count
    normed = normed.reshape(length, width)
    offset = jnp.transpose(offset, (0, 2, 1)).reshape(length, -1)
    projected = jnp.concatenate(
        [
            jnp.dot(
                normed, rows.reshape(width, -1), preferred_element_type=jnp.float32
            ).astype(jnp.bfloat16)
            for rows in (mix_rows, stick_rows)
        ],
        axis=1,
    )
    acts = []
    start = 0
    for w in widths:
        acts.append(projected[:, start : start + w])
        start += w
    gate_act, input_act, bkey_act, cquery_act, queries, key_act, value_act = acts
    input_width = input_act.shape[1]
    group_cols = bkey_act.shape[1]
    heads_local = input_width // HEAD_DIM
    groups_local = group_cols // STATE
    head_ratio = heads_local // groups_local
    blocks_local = length // BLOCK

    def conv(act, first):
        taps = lax.dynamic_slice_in_dim(
            conv_weight, first + place * act.shape[1], act.shape[1], 1
        )
        return short_conv(jnp.zeros((CONV - 1, act.shape[1]), act.dtype), act, taps)

    input_conv = conv(input_act, 0)
    bkey_conv = conv(bkey_act, SSD_INNER)
    cquery_conv = conv(cquery_act, SSD_INNER + GROUP_WIDTH)
    step_cols = lax.dynamic_slice_in_dim(w_step, place * heads_local, heads_local, 1)
    step_size = jax.nn.softplus(jnp.dot(normed, step_cols, preferred_element_type=jnp.float32))
    rate_slice = lax.dynamic_slice_in_dim(decay_rate, place * heads_local, heads_local, 0)
    log_decay = offset - rate_slice * step_size
    input_blocks = input_conv.reshape(blocks_local, BLOCK, groups_local, head_ratio, HEAD_DIM)
    bkey_blocks = bkey_conv.reshape(blocks_local, BLOCK, groups_local, STATE)
    cquery_blocks = cquery_conv.reshape(blocks_local, BLOCK, groups_local, STATE)
    step_blocks = step_size.reshape(blocks_local, BLOCK, groups_local, head_ratio)
    decay_blocks = log_decay.reshape(blocks_local, BLOCK, groups_local, head_ratio)
    cumulative, y_inner, states = block_terms(
        input_blocks, bkey_blocks, cquery_blocks, step_blocks, decay_blocks
    )
    _, entering = chain_blocks(states, cumulative[:, -1])
    y_total = y_inner + carried_output(cquery_blocks, entering, cumulative)
    gain_slice = lax.dynamic_slice_in_dim(ssd_gain, place * input_width, input_width, 0)
    y_mixer = gating_rescaled_output(
        y_total.reshape(length, groups_local, head_ratio, HEAD_DIM),
        gate_act,
        gain_slice,
        groups_local,
    )
    heads_stick = queries.shape[1] // SB_DIM
    bias_heads = lax.dynamic_slice_in_dim(stick_bias, place * heads_stick, heads_stick, 0)
    y_attend = stick_heads(
        queries.reshape(length, heads_stick, SB_DIM),
        key_act.reshape(length, heads_stick, SB_DIM),
        value_act.reshape(length, heads_stick, SB_DIM),
        bias_heads,
    ).reshape(length, heads_stick * SB_DIM)
    return scatter_sum(
        seq_count,
        lax.axis_size("tp"),
        y_mixer.reshape(seq_count, row_count, -1),
        y_attend.reshape(seq_count, row_count, -1),
        out_rows,
    )[None]


def by_heads(mesh):
    groups = GROUP_WIDTH // STATE
    fits = groups % (mesh.shape["tp"] * mesh.shape["sp"]) == 0
    return fits and mesh.shape["tp"] == 2 and mesh.shape["fs"] == 4


def solution(mesh):
    return jax.shard_map(
        head_body if by_heads(mesh) else body,
        mesh=mesh,
        in_specs=(
            P("fs", "sp", None),
            P(),
            P(("sp", "fs"), "tp"),
            P(("sp", "fs"), "tp"),
            P(("sp", "fs"), "tp"),
            P(("sp", "fs"), "tp"),
            P(),
            P(),
            P(),
            P("fs", "sp", "tp"),
            P(),
            P(("sp", "fs"), "tp"),
            P(("sp", "fs"), "tp"),
            P(("sp", "fs"), "tp"),
            P(),
            P("tp", ("sp", "fs")),
            P("tp", ("sp", "fs")),
        ),
        out_specs=P("fs", ("sp", "tp"), None),
        check_vma=False,
    )
```

```python
import functools

import jax
import jax.numpy as jnp
from jax import lax
from jax.experimental import pallas as pl
from jax.experimental.pallas import tpu as pltpu
from jax.sharding import PartitionSpec as P

HEAD_DIM = 64
STATE = 128
CONV = 4
BLOCK = 128
SB_DIM = 128
SSD_INNER = 2048
GROUP_WIDTH = 1024


EPS = 1e-06


def passed_along(shard, axis, by):
    length = lax.axis_size(axis)
    pairs = [(i, i + by) for i in range(length) if 0 <= i + by < length]
    return lax.ppermute(shard, axis, pairs)


def prefix(shard, axis, join, neutral):
    place = lax.axis_index(axis)
    gathered = jax.tree.map(
        lambda a, kind: lax.all_gather(a.astype(kind), axis), shard, (jnp.bfloat16, jnp.bfloat16)
    )
    state = jax.tree.map(lambda a, e: jnp.zeros_like(a) + jnp.asarray(e, a.dtype), shard, neutral)

    def one(step, state):
        return join(
            state,
            jax.tree.map(
                lambda a, own: lax.dynamic_index_in_dim(a, step, 0, False).astype(own.dtype),
                gathered,
                shard,
            ),
        )

    return lax.fori_loop(0, place, one, state)


def short_conv(rim_rows, current, weights):
    padded = jnp.concatenate([rim_rows, current], axis=0).astype(jnp.float32)
    length = current.shape[0]
    summed = weights[0] * padded[0:length]
    for tap_index in range(1, weights.shape[0]):
        summed = summed + weights[tap_index] * padded[tap_index : tap_index + length]
    return jax.nn.silu(summed).astype(jnp.bfloat16)


def block_terms(input_blocks, bkey_blocks, cquery_blocks, step_blocks, decay_blocks):
    cumulative = jnp.cumsum(decay_blocks, axis=1)
    cum_turned = jnp.transpose(cumulative, (0, 2, 3, 1))
    step_turned = jnp.transpose(step_blocks, (0, 2, 3, 1))
    length = input_blocks.shape[1]
    row_index = lax.broadcasted_iota(jnp.int32, (length, length), 0)
    col_index = lax.broadcasted_iota(jnp.int32, (length, length), 1)
    lower_mask = row_index >= col_index
    spread = cum_turned[..., :, None] - cum_turned[..., None, :]
    inner_prod = jnp.einsum(
        "blgn,bsgn->bgls", cquery_blocks, bkey_blocks, preferred_element_type=jnp.float32
    )
    mixing = jnp.where(
        lower_mask,
        inner_prod[:, :, None]
        * jnp.exp(jnp.where(lower_mask, spread, 0.0))
        * step_turned[..., None, :],
        0.0,
    )
    y_inner = jnp.einsum(
        "bgrls,bsgrp->blgrp",
        mixing.astype(jnp.bfloat16),
        input_blocks,
        preferred_element_type=jnp.float32,
    )
    to_end = jnp.exp(cumulative[:, -1:] - cumulative) * step_blocks
    weighted = (bkey_blocks.astype(jnp.float32)[:, :, :, None, :] * to_end[..., None]).astype(
        jnp.bfloat16
    )
    states = jnp.einsum(
        "blgrp,blgrn->bgrpn", input_blocks, weighted, preferred_element_type=jnp.float32
    )
    return (cumulative, y_inner, states)


def chain_blocks(states, totals):

    def advance(held_state, block_item):
        block_state, block_log = block_item
        return (held_state * jnp.exp(block_log)[..., None, None] + block_state, held_state)

    return lax.scan(advance, jnp.zeros_like(states[0]), (states, totals))


def carried_output(cquery_blocks, entering, cumulative):
    return (
        jnp.einsum(
            "blgn,bgrpn->blgrp",
            cquery_blocks.astype(jnp.float32),
            entering,
            precision=lax.Precision.HIGHEST,
        )
        * jnp.exp(cumulative)[..., None]
    )


def gating_rescaled_output(y_total, gate_act, gain_slice, groups):
    length = y_total.shape[0]
    group_width = y_total.shape[2] * y_total.shape[3]
    gated_out = y_total.reshape(length, groups, group_width) * jax.nn.silu(
        gate_act.astype(jnp.float32)
    ).reshape(length, groups, group_width)
    scaled = gated_out * lax.rsqrt(jnp.mean(gated_out * gated_out, axis=-1, keepdims=True) + EPS)
    return (scaled.reshape(length, groups * group_width) * gain_slice).astype(jnp.bfloat16)


def join_states(earlier, following):
    return (
        earlier[0] * jnp.exp(following[1])[..., None, None] + following[0],
        earlier[1] + following[1],
    )


def stick_piece(carried, query_heads, key_heads, value_heads, bias_heads, causal):
    summed, later_log = carried
    length = query_heads.shape[0]
    key_count = key_heads.shape[0]
    logits = (
        jnp.einsum("thd,shd->hts", query_heads, key_heads, preferred_element_type=jnp.float32)
        * query_heads.shape[2] ** (-0.5)
        + bias_heads[:, None, None]
    )
    log_keep = jax.nn.log_sigmoid(logits)
    log_pass = jax.nn.log_sigmoid(-logits)
    if causal:
        query_pos = lax.broadcasted_iota(jnp.int32, (length, key_count), 0)
        key_pos = lax.broadcasted_iota(jnp.int32, (length, key_count), 1)
        before = key_pos < query_pos
        log_pass = jnp.where(before, log_pass, 0.0)
    tail_sum = lax.cumsum(log_pass, axis=2, reverse=True) - log_pass
    weights = jnp.exp(log_keep + tail_sum + later_log[:, :, None])
    if causal:
        weights = jnp.where(before, weights, 0.0)
    summed = summed + jnp.einsum(
        "hts,shd->thd",
        weights.astype(jnp.bfloat16),
        value_heads,
        preferred_element_type=jnp.float32,
    )
    return (summed, later_log + jnp.sum(log_pass, axis=2))


def body(
    inputs,
    norm_gain,
    w_gate,
    w_input,
    w_bkey,
    w_cquery,
    w_step,
    conv_weight,
    decay_rate,
    decay_offset,
    ssd_gain,
    w_query,
    w_key,
    w_value,
    stick_bias,
    out_mixer,
    out_attend,
):
    tensor_index = lax.axis_index("tp")
    seq_index = lax.axis_index("sp")
    seq_count = lax.axis_size("sp")
    tokens = inputs[0]
    row_count = tokens.shape[0]
    widened = tokens.astype(jnp.float32)
    normed = (
        widened * lax.rsqrt(jnp.mean(widened * widened, axis=-1, keepdims=True) + EPS) * norm_gain
    ).astype(jnp.bfloat16)
    pieces = (
        lax.all_gather(w_gate, ("sp", "fs"), axis=0, tiled=True),
        lax.all_gather(w_input, ("sp", "fs"), axis=0, tiled=True),
        lax.all_gather(w_bkey, ("sp", "fs"), axis=0, tiled=True),
        lax.all_gather(w_cquery, ("sp", "fs"), axis=0, tiled=True),
        lax.all_gather(w_query, ("sp", "fs"), axis=0, tiled=True),
        lax.all_gather(w_key, ("sp", "fs"), axis=0, tiled=True),
        lax.all_gather(w_value, ("sp", "fs"), axis=0, tiled=True),
    )
    projected = tuple(
        (jnp.dot(normed, piece_rows, preferred_element_type=jnp.float32) for piece_rows in pieces)
    )
    gate_act, input_act, input_projection_after_silu, cquery_act, queries, key_act, value_act = (
        tuple((summed.astype(jnp.bfloat16) for summed in projected))
    )
    mixer_full, attend_full = (
        lax.all_gather(out_mixer, ("sp", "fs"), axis=1, tiled=True),
        lax.all_gather(out_attend, ("sp", "fs"), axis=1, tiled=True),
    )
    input_width = input_act.shape[1]
    group_cols = input_projection_after_silu.shape[1]
    heads_local = input_width // HEAD_DIM
    groups_local = group_cols // STATE
    head_ratio = heads_local // groups_local
    blocks_local = row_count // BLOCK
    rim_input, rim_bkey, rim_cquery = passed_along(
        (
            input_act[row_count - CONV + 1 :],
            input_projection_after_silu[row_count - CONV + 1 :],
            cquery_act[row_count - CONV + 1 :],
        ),
        "sp",
        1,
    )
    conv_input = lax.dynamic_slice_in_dim(conv_weight, tensor_index * input_width, input_width, 1)
    conv_bkey = lax.dynamic_slice_in_dim(
        conv_weight, SSD_INNER + tensor_index * group_cols, group_cols, 1
    )
    conv_cquery = lax.dynamic_slice_in_dim(
        conv_weight, SSD_INNER + GROUP_WIDTH + tensor_index * group_cols, group_cols, 1
    )
    input_conv = short_conv(rim_input, input_act, conv_input)
    bkey_conv = short_conv(rim_bkey, input_projection_after_silu, conv_bkey)
    cquery_conv = short_conv(rim_cquery, cquery_act, conv_cquery)
    step_cols = lax.dynamic_slice_in_dim(w_step, tensor_index * heads_local, heads_local, 1)
    step_size = jax.nn.softplus(jnp.dot(normed, step_cols, preferred_element_type=jnp.float32))
    rate_slice = lax.dynamic_slice_in_dim(decay_rate, tensor_index * heads_local, heads_local, 0)
    log_decay = decay_offset[0] - rate_slice * step_size
    input_blocks = input_conv.reshape(blocks_local, BLOCK, groups_local, head_ratio, HEAD_DIM)
    bkey_blocks = bkey_conv.reshape(blocks_local, BLOCK, groups_local, STATE)
    cquery_blocks = cquery_conv.reshape(blocks_local, BLOCK, groups_local, STATE)
    step_blocks = step_size.reshape(blocks_local, BLOCK, groups_local, head_ratio)
    decay_blocks = log_decay.reshape(blocks_local, BLOCK, groups_local, head_ratio)
    cumulative, y_inner, states = block_terms(
        input_blocks, bkey_blocks, cquery_blocks, step_blocks, decay_blocks
    )
    totals = cumulative[:, -1]
    local_end, local_entering = chain_blocks(states, totals)
    device_log = jnp.sum(totals, axis=0)
    carried_state, carried_log = prefix(
        (local_end, device_log),
        "sp",
        join_states,
        (jnp.zeros_like(local_end), jnp.zeros_like(device_log)),
    )
    before_log = jnp.cumsum(totals, axis=0) - totals
    entering = local_entering + jnp.exp(before_log)[..., None, None] * carried_state[None]
    y_total = y_inner + carried_output(cquery_blocks, entering, cumulative)
    gain_slice = lax.dynamic_slice_in_dim(ssd_gain, tensor_index * input_width, input_width, 0)
    y_mixer = gating_rescaled_output(
        y_total.reshape(row_count, groups_local, head_ratio, HEAD_DIM),
        gate_act,
        gain_slice,
        groups_local,
    )
    heads_stick = queries.shape[1] // SB_DIM
    query_heads = queries.reshape(row_count, heads_stick, SB_DIM)
    key_heads = key_act.reshape(row_count, heads_stick, SB_DIM)
    value_heads = value_act.reshape(row_count, heads_stick, SB_DIM)
    bias_heads = lax.dynamic_slice_in_dim(stick_bias, tensor_index * heads_stick, heads_stick, 0)
    carried = (
        jnp.zeros((row_count, heads_stick, SB_DIM), jnp.float32),
        jnp.zeros((heads_stick, row_count), jnp.float32),
    )
    carried = stick_piece(carried, query_heads, key_heads, value_heads, bias_heads, True)

    def relay(turn_index, held_four):
        summed, later_log, key_here, value_here = held_four
        key_here, value_here = passed_along((key_here, value_here), "sp", 1)

        def take_piece(retained_couple):
            return stick_piece(
                retained_couple, query_heads, key_here, value_here, bias_heads, False
            )

        def skip_piece(retained_couple):
            return retained_couple

        summed, later_log = lax.cond(
            turn_index < seq_index, take_piece, skip_piece, (summed, later_log)
        )
        return (summed, later_log, key_here, value_here)

    outcome = lax.fori_loop(
        0, seq_count - 1, relay, (carried[0], carried[1], key_heads, value_heads)
    )
    carried = (outcome[0], outcome[1])
    y_attend = carried[0].astype(jnp.bfloat16).reshape(row_count, heads_stick * SB_DIM)
    mixed = lax.psum_scatter(
        (
            jnp.dot(y_mixer, mixer_full, preferred_element_type=jnp.float32)
            + jnp.dot(y_attend, attend_full, preferred_element_type=jnp.float32)
        ).astype(jnp.bfloat16),
        "tp",
        scatter_dimension=0,
        tiled=True,
    )
    return mixed[None]


MESH = pl.DeviceIdType.MESH


def remote(src, dst, send, recv, **where):
    return pltpu.make_async_remote_copy(
        src_ref=src,
        dst_ref=dst,
        send_sem=send,
        recv_sem=recv,
        device_id=where,
        device_id_type=MESH,
    )


def partner(place, mask, count):
    found, bit = 0, 1
    while bit < count:
        own = lax.rem(lax.div(place, bit), 2)
        found = found + bit * (1 - own if mask & bit else own)
        bit *= 2
    return found


def partner_order(count):
    return list(range((count + 1) // 2, count)) + list(range(1, (count + 1) // 2))


def greet(seq_count, fs_peers):
    barrier = pltpu.get_barrier_semaphore()
    s = lax.axis_index("sp")
    peers = [{"tp": 1 - lax.axis_index("tp")}]
    peers += [{"sp": lax.rem(s + d, seq_count)} for d in range(1, seq_count)]
    peers += [{"fs": peer} for peer in fs_peers]
    for peer in peers:
        pl.semaphore_signal(barrier, inc=1, device_id=peer, device_id_type=MESH)
    pl.semaphore_wait(barrier, len(peers))


def gather_kernel(
    seq_count,
    batch_count,
    gate,
    inp,
    bkey,
    cquery,
    query,
    key,
    value,
    mixer,
    attend,
    normed,
    offset,
    mix_rows,
    stick_rows,
    out_rows,
    all_normed,
    all_offset,
    own_sem,
    z_send,
    z_recv,
    f_send,
    f_recv,
    h_send,
    h_recv,
    n_send,
    n_recv,
    p_send,
    p_recv,
    o_send,
    o_recv,
    last_sem,
):
    s, f, t = lax.axis_index("sp"), lax.axis_index("fs"), lax.axis_index("tp")
    row_x = lax.rem(f, 2)
    across = f + 1 - 2 * row_x
    along = lax.rem(f + 2, 4)
    greet(seq_count, (across, along))
    depth = gate.shape[0]
    piece_cols = out_rows.shape[1] // (seq_count * batch_count)
    half_rows = normed.shape[0] // 2

    def column_pieces(arrays):
        found, at = [], 0
        for ref in arrays:
            found.append((ref, at, ref.shape[1] // seq_count))
            at += found[-1][2]
        return found

    def row_pieces(arrays):
        found, at = [], 0
        for ref in arrays:
            found.append((ref, at, ref.shape[0] // seq_count))
            at += found[-1][2]
        return found

    kinds = (
        (mix_rows, column_pieces((gate, inp, bkey, cquery)), False),
        (stick_rows, column_pieces((query, key, value)), False),
        (out_rows, row_pieces((mixer, attend)), True),
    )

    def chunk(kind, from_s, from_f):
        dest, _, by_rows = kinds[kind]
        if by_rows:
            at = pl.multiple_of((from_s * batch_count + from_f) * piece_cols, piece_cols)
            return dest.at[:, pl.ds(at, piece_cols)]
        return dest.at[from_s, from_f]

    def half(kind, from_s, from_f, which):
        dest, _, by_rows = kinds[kind]
        if by_rows:
            rows = dest.shape[0] // 2
            at = pl.multiple_of((from_s * batch_count + from_f) * piece_cols, piece_cols)
            return dest.at[pl.ds(which * rows, rows), pl.ds(at, piece_cols)]
        rows = depth // 2
        return dest.at[from_s, from_f, pl.ds(which * rows, rows)]

    def piece(kind, number, to_s, from_s):
        dest, found, by_rows = kinds[kind]
        ref, at, size = found[number]
        start = pl.multiple_of(to_s * size, size)
        if by_rows:
            column = pl.multiple_of((from_s * batch_count + f) * piece_cols, piece_cols)
            return (
                ref.at[pl.ds(start, size), :],
                dest.at[pl.ds(at, size), pl.ds(column, piece_cols)],
            )
        return ref.at[:, pl.ds(start, size)], dest.at[from_s, f, :, pl.ds(at, size)]

    base = []
    total = 0
    for kind in range(3):
        base.append(total)
        total += len(kinds[kind][1])
    sent = []

    def begin(copy):
        copy.start()
        sent.append(copy)

    own = [[] for _ in range(3)]
    for kind in range(3):
        for number in range(len(kinds[kind][1])):
            source, dest = piece(kind, number, s, s)
            copy = pltpu.make_async_copy(source, dest, own_sem.at[base[kind] + number])
            copy.start()
            own[kind].append(copy)
    keep_normed = pltpu.make_async_copy(normed, all_normed.at[s], last_sem.at[0])
    keep_normed.start()
    keep_offset = pltpu.make_async_copy(offset.at[s], all_offset.at[s], last_sem.at[1])
    keep_offset.start()

    order = partner_order(seq_count)

    def send_kind(kind):
        for d in order:
            q = partner(s, d, seq_count)
            for number in range(len(kinds[kind][1])):
                source, dest = piece(kind, number, q, s)
                at = base[kind] + number
                begin(remote(source, dest, z_send.at[at, d], z_recv.at[at, d], sp=q))

    def rows_of(from_s, which):
        return all_normed.at[from_s, pl.ds(pl.multiple_of(which * half_rows, half_rows), half_rows)]

    for kind in range(3):
        send_kind(kind)
    for d in order:
        q = partner(s, d, seq_count)
        source = normed.at[pl.ds(pl.multiple_of(t * half_rows, half_rows), half_rows)]
        if d & (d - 1) == 0:
            begin(remote(source, rows_of(s, t), n_send.at[d], n_recv.at[d], sp=q))
        begin(remote(offset.at[q], all_offset.at[s], o_send.at[d], o_recv.at[d], sp=q))

    def from_of(d):
        return partner(s, d, seq_count)

    def spread(kind, d):
        from_s = from_of(d)
        if d == 0:
            for copy in own[kind]:
                copy.wait()
        else:
            for number in range(len(kinds[kind][1])):
                source, dest = piece(kind, number, s, from_s)
                at = base[kind] + number
                remote(source, dest, z_send.at[at, d], z_recv.at[at, d], sp=s).wait_recv()
        block = chunk(kind, from_s, f)
        begin(
            remote(block, block, f_send.at[kind, d, 0], f_recv.at[kind, d, 0], fs=across)
        )
        begin(
            remote(block, block, f_send.at[kind, d, 1], f_recv.at[kind, d, 1], fs=along)
        )

    def forward(kind, d):
        from_s = from_of(d)
        for which, (origin, target) in enumerate(((across, along), (along, across))):
            block = chunk(kind, from_s, origin)
            remote(
                block, block, f_send.at[kind, d, which], f_recv.at[kind, d, which], fs=origin
            ).wait_recv()
            part = half(kind, from_s, origin, which)
            begin(
                remote(
                    part, part, h_send.at[kind, d, which], h_recv.at[kind, d, which], fs=target
                )
            )

    def arrive(kind):
        opposite = 3 - f
        for d in range(seq_count):
            for which in range(2):
                part = half(kind, from_of(d), opposite, which)
                remote(
                    part, part, h_send.at[kind, d, which], h_recv.at[kind, d, which], fs=across
                ).wait_recv()

    def share_normed():
        for d in sorted(order, key=lambda d: (d & (d - 1) != 0, -d)):
            block = rows_of(from_of(d), t)
            remote(block, block, n_send.at[d], n_recv.at[d], sp=s).wait_recv()
            for bit in (1, 2):
                if d > bit and d & (d - 1) == 0 and d + bit < seq_count:
                    q = partner(s, bit, seq_count)
                    at = d + bit
                    begin(remote(block, block, n_send.at[at], n_recv.at[at], sp=q))
            begin(remote(block, block, p_send.at[d], p_recv.at[d], tp=1 - t))

    before = None
    steps = [(kind, 0) for kind in range(3)]
    steps += [(kind, d) for kind in range(3) for d in order]
    for step in steps:
        spread(*step)
        if before is not None:
            forward(*before)
        before = step
    forward(*before)
    share_normed()
    for d in range(1, seq_count):
        block = rows_of(from_of(d), 1 - t)
        remote(block, block, p_send.at[d], p_recv.at[d], tp=1 - t).wait_recv()
        remote(
            offset.at[s], all_offset.at[from_of(d)], o_send.at[d], o_recv.at[d], sp=s
        ).wait_recv()
    keep_normed.wait()
    keep_offset.wait()
    for kind in range(3):
        arrive(kind)
    for copy in sent:
        copy.wait_send()


def gather_all(seq_count, batch_count, weights, outs, normed, offset):
    depth = weights[0].shape[0]
    mix = sum(w.shape[1] for w in weights[:4]) // seq_count
    stick = sum(w.shape[1] for w in weights[4:]) // seq_count
    rows = sum(w.shape[0] for w in outs) // seq_count
    columns = outs[0].shape[1] * seq_count * batch_count
    number = len(weights) + len(outs)
    dma = pltpu.SemaphoreType.DMA
    vmem = pl.BlockSpec(memory_space=pltpu.VMEM)
    return pl.pallas_call(
        functools.partial(gather_kernel, seq_count, batch_count),
        out_shape=(
            jax.ShapeDtypeStruct((seq_count, batch_count, depth, mix), jnp.bfloat16),
            jax.ShapeDtypeStruct((seq_count, batch_count, depth, stick), jnp.bfloat16),
            jax.ShapeDtypeStruct((rows, columns), jnp.bfloat16),
            jax.ShapeDtypeStruct((seq_count,) + normed.shape, jnp.bfloat16),
            jax.ShapeDtypeStruct(offset.shape, jnp.float32),
        ),
        in_specs=[pl.BlockSpec(memory_space=pltpu.HBM)] * (number + 2),
        out_specs=(vmem,) * 5,
        scratch_shapes=[
            dma((number,)),
            dma((number, seq_count)),
            dma((number, seq_count)),
            dma((3, seq_count, 2)),
            dma((3, seq_count, 2)),
            dma((3, seq_count, 2)),
            dma((3, seq_count, 2)),
            dma((seq_count,)),
            dma((seq_count,)),
            dma((seq_count,)),
            dma((seq_count,)),
            dma((seq_count,)),
            dma((seq_count,)),
            dma((2,)),
        ],
        compiler_params=pltpu.CompilerParams(collective_id=0, has_side_effects=True),
    )(*weights, *outs, normed, offset)


def scatter_kernel(
    seq_count,
    mixer,
    attend,
    rows,
    out,
    share,
    pair,
    joined,
    land,
    p_send,
    p_recv,
    z_send,
    z_recv,
):
    s, t = lax.axis_index("sp"), lax.axis_index("tp")
    greet(seq_count, ())
    order = partner_order(seq_count) + [0]
    width = mixer.shape[2]
    sent = []
    for d in order:
        q = partner(s, d, seq_count)
        summed = jnp.dot(mixer[q], rows[:width], preferred_element_type=jnp.float32)
        summed += jnp.dot(attend[q], rows[width:], preferred_element_type=jnp.float32)
        share[d] = summed.astype(jnp.bfloat16).reshape(share.shape[1:])
        copy = remote(share.at[d, 1 - t], pair.at[d], p_send.at[d], p_recv.at[d], tp=1 - t)
        copy.start()
        sent.append(copy)
    for number, d in enumerate(order):
        q = partner(s, d, seq_count)
        sent[number].wait_recv()
        both = share[d, t].astype(jnp.float32) + pair[d].astype(jnp.float32)
        joined[d] = both.astype(jnp.bfloat16)
        if d:
            copy = remote(joined.at[d], land.at[d], z_send.at[d], z_recv.at[d], sp=q)
            copy.start()
            sent.append(copy)
    total = joined[0].astype(jnp.float32)
    for d in range(1, seq_count):
        remote(joined.at[d], land.at[d], z_send.at[d], z_recv.at[d], sp=s).wait_recv()
        total = total + land[d].astype(jnp.float32)
    out[...] = total.astype(jnp.bfloat16)
    for copy in sent:
        copy.wait_send()


def scatter_sum(seq_count, tensor_count, mixer, attend, rows):
    block = (mixer.shape[1] // tensor_count, rows.shape[1])
    vmem = pl.BlockSpec(memory_space=pltpu.VMEM)
    dma = pltpu.SemaphoreType.DMA
    return pl.pallas_call(
        functools.partial(scatter_kernel, seq_count),
        out_shape=jax.ShapeDtypeStruct(block, jnp.bfloat16),
        in_specs=[vmem] * 3,
        out_specs=vmem,
        scratch_shapes=[pltpu.VMEM((seq_count, tensor_count) + block, jnp.bfloat16)]
        + [pltpu.VMEM((seq_count,) + block, jnp.bfloat16)] * 3
        + [dma((seq_count,))] * 4,
        compiler_params=pltpu.CompilerParams(collective_id=1, has_side_effects=True),
    )(mixer, attend, rows)


def stick_heads(query_heads, key_heads, value_heads, bias_heads):
    length = query_heads.shape[0]
    logits = (
        jnp.einsum("thd,shd->hts", query_heads, key_heads, preferred_element_type=jnp.float32)
        * query_heads.shape[2] ** (-0.5)
        + bias_heads[:, None, None]
    )
    row_index = lax.broadcasted_iota(jnp.int32, (length, length), 0)
    col_index = lax.broadcasted_iota(jnp.int32, (length, length), 1)
    before = col_index < row_index
    log_keep = jax.nn.log_sigmoid(logits)
    log_pass = jnp.where(before, log_keep - logits, 0.0)
    later = (row_index > col_index).astype(jnp.float32)
    tail_sum = jnp.einsum("htr,rs->hts", log_pass, later, precision=lax.Precision.HIGH)
    weights = jnp.where(before, jnp.exp(log_keep + tail_sum), 0.0)
    return jnp.einsum(
        "hts,shd->thd",
        weights.astype(jnp.bfloat16),
        value_heads,
        preferred_element_type=jnp.float32,
    ).astype(jnp.bfloat16)


def head_body(
    inputs,
    norm_gain,
    w_gate,
    w_input,
    w_bkey,
    w_cquery,
    w_step,
    conv_weight,
    decay_rate,
    decay_offset,
    ssd_gain,
    w_query,
    w_key,
    w_value,
    stick_bias,
    out_mixer,
    out_attend,
):
    seq_count = lax.axis_size("sp")
    batch_count = lax.axis_size("fs")
    place = lax.axis_index("tp") * seq_count + lax.axis_index("sp")
    tokens = inputs[0]
    row_count, width = tokens.shape
    widened = tokens.astype(jnp.float32)
    normed = (
        widened * lax.rsqrt(jnp.mean(widened * widened, axis=-1, keepdims=True) + EPS) * norm_gain
    ).astype(jnp.bfloat16)
    weights = (w_gate, w_input, w_bkey, w_cquery, w_query, w_key, w_value)
    widths = [w.shape[1] // seq_count for w in weights]
    offset = jnp.transpose(decay_offset[0]).reshape(seq_count, -1, row_count)
    mix_rows, stick_rows, out_rows, normed, offset = gather_all(
        seq_count, batch_count, weights, (out_mixer, out_attend), normed, offset
    )
    length = seq_count * row_count
    normed = normed.reshape(length, width)
    offset = jnp.transpose(offset, (0, 2, 1)).reshape(length, -1)
    projected = jnp.concatenate(
        [
            jnp.dot(
                normed, rows.reshape(width, -1), preferred_element_type=jnp.float32
            ).astype(jnp.bfloat16)
            for rows in (mix_rows, stick_rows)
        ],
        axis=1,
    )
    acts = []
    start = 0
    for w in widths:
        acts.append(projected[:, start : start + w])
        start += w
    gate_act, input_act, bkey_act, cquery_act, queries, key_act, value_act = acts
    input_width = input_act.shape[1]
    group_cols = bkey_act.shape[1]
    heads_local = input_width // HEAD_DIM
    groups_local = group_cols // STATE
    head_ratio = heads_local // groups_local
    blocks_local = length // BLOCK

    def conv(act, first):
        taps = lax.dynamic_slice_in_dim(
            conv_weight, first + place * act.shape[1], act.shape[1], 1
        )
        return short_conv(jnp.zeros((CONV - 1, act.shape[1]), act.dtype), act, taps)

    input_conv = conv(input_act, 0)
    bkey_conv = conv(bkey_act, SSD_INNER)
    cquery_conv = conv(cquery_act, SSD_INNER + GROUP_WIDTH)
    step_cols = lax.dynamic_slice_in_dim(w_step, place * heads_local, heads_local, 1)
    step_size = jax.nn.softplus(jnp.dot(normed, step_cols, preferred_element_type=jnp.float32))
    rate_slice = lax.dynamic_slice_in_dim(decay_rate, place * heads_local, heads_local, 0)
    log_decay = offset - rate_slice * step_size
    input_blocks = input_conv.reshape(blocks_local, BLOCK, groups_local, head_ratio, HEAD_DIM)
    bkey_blocks = bkey_conv.reshape(blocks_local, BLOCK, groups_local, STATE)
    cquery_blocks = cquery_conv.reshape(blocks_local, BLOCK, groups_local, STATE)
    step_blocks = step_size.reshape(blocks_local, BLOCK, groups_local, head_ratio)
    decay_blocks = log_decay.reshape(blocks_local, BLOCK, groups_local, head_ratio)
    cumulative, y_inner, states = block_terms(
        input_blocks, bkey_blocks, cquery_blocks, step_blocks, decay_blocks
    )
    _, entering = chain_blocks(states, cumulative[:, -1])
    y_total = y_inner + carried_output(cquery_blocks, entering, cumulative)
    gain_slice = lax.dynamic_slice_in_dim(ssd_gain, place * input_width, input_width, 0)
    y_mixer = gating_rescaled_output(
        y_total.reshape(length, groups_local, head_ratio, HEAD_DIM),
        gate_act,
        gain_slice,
        groups_local,
    )
    heads_stick = queries.shape[1] // SB_DIM
    bias_heads = lax.dynamic_slice_in_dim(stick_bias, place * heads_stick, heads_stick, 0)
    y_attend = stick_heads(
        queries.reshape(length, heads_stick, SB_DIM),
        key_act.reshape(length, heads_stick, SB_DIM),
        value_act.reshape(length, heads_stick, SB_DIM),
        bias_heads,
    ).reshape(length, heads_stick * SB_DIM)
    return scatter_sum(
        seq_count,
        lax.axis_size("tp"),
        y_mixer.reshape(seq_count, row_count, -1),
        y_attend.reshape(seq_count, row_count, -1),
        out_rows,
    )[None]


def by_heads(mesh):
    groups = GROUP_WIDTH // STATE
    fits = groups % (mesh.shape["tp"] * mesh.shape["sp"]) == 0
    return fits and mesh.shape["tp"] == 2 and mesh.shape["fs"] == 4 and mesh.shape["sp"] <= 4


def solution(mesh):
    return jax.shard_map(
        head_body if by_heads(mesh) else body,
        mesh=mesh,
        in_specs=(
            P("fs", "sp", None),
            P(),
            P(("sp", "fs"), "tp"),
            P(("sp", "fs"), "tp"),
            P(("sp", "fs"), "tp"),
            P(("sp", "fs"), "tp"),
            P(),
            P(),
            P(),
            P("fs", "sp", "tp"),
            P(),
            P(("sp", "fs"), "tp"),
            P(("sp", "fs"), "tp"),
            P(("sp", "fs"), "tp"),
            P(),
            P("tp", ("sp", "fs")),
            P("tp", ("sp", "fs")),
        ),
        out_specs=P("fs", ("sp", "tp"), None),
        check_vma=False,
    )
```
